32 devices in a mesh: gr: 2 (over y), sp: 4 (over z), tp: 4 (over x, core).
Axes of the slice: x: 2, y: 2, z: 4, core: 2. Of those that a mesh axis runs over, the one named last changes fastest.
Arguments:
- layer_input: bfloat16 [2, 3072, 2048], P('gr', ('sp', 'tp')), may hold values from -6 to 6
- key_weight: bfloat16 [2048, 2048], P(None, 'tp'), may hold values from -0.125 to 0.125
- value_weight: bfloat16 [2048, 2048], P(None, 'tp'), may hold values from -0.125 to 0.125
- new_queries: bfloat16 [2, 2048], P('gr', 'tp'), may hold values from -280 to 280
- lambdas: float32 [16], P('tp'), may hold values from 0.3 to 0.8
- head_gain: float32 [128], replicated, may hold values from 0.1 to 1.9
- out_weight: bfloat16 [2048, 2048], P('tp'), may hold values from -0.125 to 0.125
Outputs:
- key_cache: bfloat16 [2, 3072, 2048], P('gr', 'sp', 'tp')
- value_cache: bfloat16 [2, 3072, 2048], P('gr', 'sp', 'tp')
- mixed: bfloat16 [2, 2048], P('gr', 'tp')
The draws below stay inside these ranges and needn't reach their ends.
All inputs are finite; a program needn't handle non-finite values.
Results may differ from the reference program's by a relative error of at most 0.03.
Values may be sent and summed in bfloat16 or wider, within the bound.
A program may use at most 64 MiB of HBM per device.

```python
import jax
import jax.numpy as jnp
from jax import lax

D = 2048
HEADS = 16
HEAD_DIM = 64
ROWS = 192
LEN = 3072
SEQS = 2
N_SP = 4
N_TP = 4


def draw_new_queries(key, part):
    drawn_rows = jax.random.normal(jax.random.fold_in(key, 11), (SEQS, HEADS * 2 * HEAD_DIM), jnp.float32)
    drawn_rows = jnp.clip(drawn_rows, -4.0, 4.0) * 1.7
    return drawn_rows.astype(jnp.bfloat16)


def block_scale(key, shape, pieces, low, high):
    factor_of, own = 1.0, jax.random.fold_in(key, 6)
    for position, parts in pieces:
        heights = jnp.exp(jax.random.uniform(jax.random.fold_in(own, position), (parts,), jnp.float32, low / len(pieces), high / len(pieces)))
        factor_of = factor_of * jnp.repeat(heights, shape[position] // parts).reshape([-1 if axis == position else 1 for axis in range(len(shape))])
    return factor_of


def gaussian(own_key, dims, scale, most, cuts=(), kind=jnp.bfloat16):
    loudness = block_scale(own_key, dims, cuts, -0.22, 0.18) if cuts else 1.0
    entries = jax.random.normal(own_key, dims, jnp.float32) * scale * loudness
    return jnp.minimum(jnp.maximum(entries, -most), most).astype(kind)


def setup_inputs(seed: int = 0) -> dict:
    arg_keys = jax.random.split(jax.random.key(seed), 8)
    return {
        "layer_input": gaussian(arg_keys[0], (SEQS, LEN, D), 1.0, 6.0, ((0, 2), (1, 16))),
        "key_weight": gaussian(arg_keys[1], (D, HEADS * 2 * HEAD_DIM), D ** -0.5, 0.125, ((1, 4),)),
        "value_weight": gaussian(arg_keys[2], (D, HEADS * 2 * HEAD_DIM), D ** -0.5, 0.125, ((1, 4),)),
        "new_queries": draw_new_queries(jax.random.fold_in(arg_keys[7], 71), 0),
        "lambdas": jnp.clip(0.3 + 0.5 * jax.random.uniform(arg_keys[4], (HEADS,), jnp.float32) ** block_scale(arg_keys[4], (HEADS,), ((0, 4),), -0.2, 0.2), 0.3, 0.8),
        "head_gain": jnp.clip(1.0 + 0.18 * jax.random.normal(arg_keys[5], (2 * HEAD_DIM,), jnp.float32), 0.1, 1.9),
        "out_weight": gaussian(arg_keys[6], (HEADS * 2 * HEAD_DIM, D), (HEADS * 2 * HEAD_DIM) ** -0.5, 0.125, ((0, 4),)),
    }


def rotate(raw_keys, positions, head_dim):
    inverse = 1.0 / 10000.0 ** (jnp.arange(0, head_dim, 2, dtype=jnp.float32) / head_dim)
    angles = positions.astype(jnp.float32)[:, None] * inverse[None, :]
    angles = jnp.concatenate([angles, angles], axis=-1)
    cosine = jnp.cos(angles)[:, None, :]
    sine = jnp.sin(angles)[:, None, :]
    first_half, second_half = jnp.split(raw_keys, 2, axis=-1)
    turned = jnp.concatenate([-second_half, first_half], axis=-1)
    return raw_keys * cosine + turned * sine

def reference(layer_input, key_weight, value_weight, new_queries, lambdas, head_gain, out_weight):
    block_rows = ROWS * N_TP
    column_count = HEADS * 2 * HEAD_DIM

    def project(items):
        block, index = items
        raw_keys = jnp.dot(block, key_weight, preferred_element_type=jnp.float32)
        raw_keys = raw_keys.reshape(block_rows, 2 * HEADS, HEAD_DIM)
        positions = index * block_rows + jnp.arange(block_rows, dtype=jnp.int32)
        key_rows = rotate(raw_keys, positions, HEAD_DIM)
        key_rows = key_rows.reshape(block_rows, column_count).astype(jnp.bfloat16)
        value_rows = jnp.dot(block, value_weight, preferred_element_type=jnp.float32).astype(jnp.bfloat16)
        return (key_rows, value_rows)
    key_list = []
    value_list = []
    read_list = []
    for seq_index in range(SEQS):
        blocks = layer_input[seq_index].reshape(N_SP, block_rows, D)
        key_blocks, value_blocks = lax.map(project, (blocks, jnp.arange(N_SP, dtype=jnp.int32)))
        key_rows = key_blocks.reshape(LEN, column_count)
        value_rows = value_blocks.reshape(LEN, column_count)
        query_row = new_queries[seq_index].astype(jnp.float32)

        def read_head(head):
            first = (head * 2 * HEAD_DIM).astype(jnp.int32)
            key_part = lax.dynamic_slice_in_dim(key_rows, first, 2 * HEAD_DIM, 1).astype(jnp.float32)
            key_part = key_part.reshape(LEN, 2, HEAD_DIM)
            value_part = lax.dynamic_slice_in_dim(value_rows, first, 2 * HEAD_DIM, 1).astype(jnp.float32)
            query_part = lax.dynamic_slice_in_dim(query_row, first, 2 * HEAD_DIM, 0).reshape(2, HEAD_DIM)
            scores = jnp.einsum('md,lmd->ml', query_part, key_part) * HEAD_DIM ** (-0.5)
            maps = jax.nn.softmax(scores, axis=-1)
            return jnp.einsum('ml,le->me', maps, value_part)
        read_list.append(lax.map(read_head, jnp.arange(HEADS, dtype=jnp.int32)))
        key_list.append(key_rows)
        value_list.append(value_rows)
    key_cache = jnp.stack(key_list, axis=0)
    value_cache = jnp.stack(value_list, axis=0)
    reads = jnp.stack(read_list, axis=0)
    diff = reads[:, :, 0] - lambdas[None, :, None] * reads[:, :, 1]
    normed = diff * lax.rsqrt(lax.optimization_barrier(jnp.mean(diff * diff, axis=-1, keepdims=True)) + 1e-06) * head_gain
    headed = normed.reshape(SEQS, column_count).astype(jnp.bfloat16)
    group_cols = column_count // N_TP
    grouped = headed.reshape(SEQS, N_TP, group_cols).astype(jnp.float32)
    weight_groups = out_weight.reshape(N_TP, group_cols, D).astype(jnp.float32)
    partials = jnp.einsum('stc,tcd->std', grouped, weight_groups).astype(jnp.bfloat16)
    mixed = lax.optimization_barrier(jnp.sum(partials.astype(jnp.float32), axis=1)).astype(jnp.bfloat16)
    return (key_cache, value_cache, mixed)
```

```python
import functools

import jax
import jax.numpy as jnp
import numpy as np
from jax import lax
from jax.experimental import pallas as pl
from jax.experimental.pallas import tpu as pltpu
from jax.sharding import PartitionSpec as P

MESH = pl.DeviceIdType.MESH
MAP_ROWS = 16
VMEM_BYTES = 67043328
SMALL_BYTES = 16384
SLICES = (3, 2, 2, 1)


def kernel(
    n_sp, n_tp, heads, head_dim, chunk,
    x_ref, wk_ref, wv_ref, q_ref, lam_ref, gain_ref, wo_ref, fine_ref, coarse_ref,
    keys, values, mix_ref,
    xg, wk, wv, wo, q, lam, gain, fine, coarse, stats, part, parts, sums,
    load_sem, own_sem, up_sem, down_sem, near_send, near_recv, far_send, far_recv, fwd_send, fwd_recv,
    st_send, st_recv, pt_send, pt_recv,
):
    sp = lax.axis_index("sp")
    tp = lax.axis_index("tp")
    rows, depth = x_ref.shape[1:]
    columns = wk.shape[1]
    wide = 2 * head_dim
    maps = 2 * heads
    steps = rows // chunk
    chips = n_tp // 2
    partner = tp + 1 - 2 * lax.rem(tp, 2)
    out_cols = mix_ref.shape[1]
    local_coarse = n_tp * steps
    last = steps - 1
    unit = depth // sum(SLICES)
    edges = [unit * sum(SLICES[:i]) for i in range(len(SLICES) + 1)]
    cuts = [slice(edges[i], edges[i + 1]) for i in range(len(SLICES))]
    pieces = [(j, slice(0, depth)) for j in range(last)] + [(last, cut) for cut in cuts]

    def piece_of(block, piece):
        j, cut = pieces[piece]
        return xg.at[block, pl.ds(j * chunk, chunk), pl.ds(cut.start, cut.stop - cut.start)]

    own_loads = [
        pltpu.make_async_copy(
            x_ref.at[0, pl.ds(j * chunk, chunk)], xg.at[tp, pl.ds(j * chunk, chunk)], own_sem.at[j]
        )
        for j in range(steps)
    ]
    loads = [
        pltpu.make_async_copy(q_ref, q, load_sem.at[5]),
        pltpu.make_async_copy(wk_ref, wk, load_sem.at[1]),
        pltpu.make_async_copy(wv_ref, wv, load_sem.at[2]),
        pltpu.make_async_copy(fine_ref, fine, load_sem.at[3]),
        pltpu.make_async_copy(
            coarse_ref.at[pl.ds(sp * local_coarse, local_coarse)], coarse, load_sem.at[4]
        ),
        pltpu.make_async_copy(lam_ref, lam, load_sem.at[6]),
        pltpu.make_async_copy(gain_ref, gain, load_sem.at[7]),
        pltpu.make_async_copy(wo_ref, wo, load_sem.at[8]),
    ]

    barrier = pltpu.get_barrier_semaphore()
    for d in range(1, n_tp):
        pl.semaphore_signal(
            barrier, inc=1, device_id={"tp": lax.rem(tp + d, n_tp)}, device_id_type=MESH
        )
    has_lower = sp > 0
    has_upper = sp < n_sp - 1

    @pl.when(has_lower)
    def _():
        pl.semaphore_signal(barrier, inc=1, device_id={"sp": sp - 1}, device_id_type=MESH)

    @pl.when(has_upper)
    def _():
        pl.semaphore_signal(barrier, inc=1, device_id={"sp": sp + 1}, device_id_type=MESH)

    for load in own_loads:
        load.start()
    pl.semaphore_wait(barrier, n_tp - 1 + jnp.where(has_lower, 1, 0) + jnp.where(has_upper, 1, 0))

    far = {}
    for p in range(len(pieces)):
        if p < steps:
            own_loads[p].wait()
        for d in range(1, chips):
            far[d, p] = pltpu.make_async_remote_copy(
                src_ref=piece_of(tp, p),
                dst_ref=piece_of(tp, p),
                send_sem=far_send.at[d - 1, p],
                recv_sem=far_recv.at[d - 1, p],
                device_id={"tp": lax.rem(tp + 2 * d, n_tp)},
                device_id_type=MESH,
            )
            far[d, p].start()
    near = pltpu.make_async_remote_copy(
        src_ref=xg.at[tp],
        dst_ref=xg.at[tp],
        send_sem=near_send,
        recv_sem=near_recv,
        device_id={"tp": partner},
        device_id_type=MESH,
    )
    near.start()
    for load in loads:
        load.start()

    lane = lax.broadcasted_iota(jnp.int32, (chunk, wide), 1)
    low_half = lax.rem(lane, head_dim) < head_dim // 2

    def settle(block, first, count, raw_keys, raw_values):
        values[block, first * chunk:(first + count) * chunk, :] = raw_values.astype(jnp.bfloat16)
        for i in range(count):
            base = coarse[block * steps + first + i]
            base_cos, base_sin = base[0:1, :], base[1:2, :]
            cosine = base_cos * fine[0] - base_sin * fine[1]
            sine = base_sin * fine[0] + base_cos * fine[1]
            for h in range(heads):
                raw = raw_keys[i * chunk:(i + 1) * chunk, h * wide:(h + 1) * wide]
                ahead = pltpu.roll(raw, wide - head_dim // 2, 1)
                behind = pltpu.roll(raw, head_dim // 2, 1)
                turned = raw * cosine + jnp.where(low_half, ahead, behind) * sine
                keys[
                    block, (first + i) * chunk:(first + i + 1) * chunk, h * wide:(h + 1) * wide
                ] = turned.astype(jnp.bfloat16)

    def product(block, first, count, cut):
        piece = xg[block, first * chunk:(first + count) * chunk, cut]
        raw_keys = jnp.dot(piece, wk[cut, :], preferred_element_type=jnp.float32)
        raw_values = jnp.dot(piece, wv[cut, :], preferred_element_type=jnp.float32)
        return raw_keys, raw_values

    def project(block, first, count):
        settle(block, first, count, *product(block, first, count, slice(0, depth)))

    for load in loads[:5]:
        load.wait()
    map_row = lax.broadcasted_iota(jnp.int32, (MAP_ROWS, columns), 0)
    map_col = lax.broadcasted_iota(jnp.int32, (MAP_ROWS, columns), 1) // head_dim
    spread = jnp.where(map_row == map_col, q[...].astype(jnp.float32), 0.0).astype(jnp.bfloat16)

    def attend(state, block, first, count):
        where = slice(first * chunk, (first + count) * chunk)
        score = lax.dot_general(
            spread, keys[block, where, :], (((1,), (1,)), ((), ())),
            preferred_element_type=jnp.float32,
        ) * head_dim ** (-0.5)
        highest = jnp.max(score, axis=1, keepdims=True)
        if state is not None:
            highest = jnp.maximum(highest, state[0])
        weight = jnp.exp(score - highest)
        total = jnp.sum(weight, axis=1, keepdims=True)
        upper = weight.astype(jnp.bfloat16)
        lower = (weight - upper.astype(jnp.float32)).astype(jnp.bfloat16)
        read = jnp.dot(
            jnp.concatenate([upper, lower], axis=0), values[block, where, :],
            preferred_element_type=jnp.float32,
        )
        read = read[:MAP_ROWS] + read[MAP_ROWS:]
        if state is not None:
            fade = jnp.exp(state[0] - highest)
            total = total + state[1] * fade
            read = read + state[2] * fade
        return highest, total, read

    project(tp, 0, steps)
    state = attend(None, tp, 0, steps)

    pl.when(has_lower)(lambda: pl.semaphore_wait(up_sem, 1))

    @pl.when(has_upper)
    def _():
        pl.semaphore_signal(up_sem, inc=1, device_id={"sp": sp + 1}, device_id_type=MESH)

    near.wait_recv()
    project(partner, 0, steps)
    state = attend(state, partner, 0, steps)

    pl.when(has_upper)(lambda: pl.semaphore_wait(down_sem, 1))

    @pl.when(has_lower)
    def _():
        pl.semaphore_signal(down_sem, inc=1, device_id={"sp": sp - 1}, device_id_type=MESH)

    for load in loads[5:]:
        load.wait()
    map_of = lax.broadcasted_iota(jnp.int32, (maps, wide), 0)
    lam_row = jnp.zeros((maps, wide), jnp.float32)
    for h in range(heads):
        lam_row = jnp.where(map_of == 2 * h, lam[0:1, h:h + 1], lam_row)

    sources = {d: lax.rem(tp + n_tp - 2 * d, n_tp) for d in range(1, chips)}
    others = {d: sources[d] + 1 - 2 * lax.rem(sources[d], 2) for d in sources}
    forwards = {}

    def forward(d, p):
        far[d, p].wait_recv()
        forwards[d, p] = pltpu.make_async_remote_copy(
            src_ref=piece_of(sources[d], p),
            dst_ref=piece_of(sources[d], p),
            send_sem=fwd_send.at[d - 1, p],
            recv_sem=fwd_recv.at[d - 1, p],
            device_id={"tp": partner},
            device_id_type=MESH,
        )
        forwards[d, p].start()

    for j in range(last):
        for d in sources:
            forward(d, j)
            project(sources[d], j, 1)
            state = attend(state, sources[d], j, 1)
            forwards[d, j].wait_recv()
            project(others[d], j, 1)
            state = attend(state, others[d], j, 1)

    def add_slice(d, side, block, i):
        raw_keys, raw_values = product(block, last, 1, cuts[i])
        slot = 2 * (d - 1) + side
        if i > 0:
            raw_keys = raw_keys + sums[slot, :, :columns]
            raw_values = raw_values + sums[slot, :, columns:]
        if i < len(cuts) - 1:
            sums[slot, :, :columns] = raw_keys
            sums[slot, :, columns:] = raw_values
        else:
            settle(block, last, 1, raw_keys, raw_values)

    final = len(cuts) - 1
    for i in range(len(cuts)):
        for d in sources:
            forward(d, last + i)
        for d in sources:
            if i > 0:
                forwards[d, last + i - 1].wait_recv()
                add_slice(d, 1, others[d], i - 1)
            add_slice(d, 0, sources[d], i)
            if i == final:
                state = attend(state, sources[d], last, 1)
    for d in sources:
        forwards[d, last + final].wait_recv()
        add_slice(d, 1, others[d], final)
        state = attend(state, others[d], last, 1)

    highest, total, read = state
    head_of = lax.broadcasted_iota(jnp.int32, (MAP_ROWS, wide), 0) // 2
    own = jnp.zeros((MAP_ROWS, wide), jnp.float32)
    for h in range(heads):
        own = jnp.where(head_of == h, read[:, h * wide:(h + 1) * wide], own)
    first_lane = lax.broadcasted_iota(jnp.int32, (MAP_ROWS, wide), 1) == 0
    stats[sp, 0] = own[:maps]
    stats[sp, 1] = jnp.where(first_lane, highest, total)[:maps]

    exchanges = []
    for d in range(n_sp - 1, 0, -1):
        copy = pltpu.make_async_remote_copy(
            src_ref=stats.at[sp],
            dst_ref=stats.at[sp],
            send_sem=st_send.at[d - 1],
            recv_sem=st_recv.at[d - 1],
            device_id={"sp": lax.rem(sp + d, n_sp)},
            device_id_type=MESH,
        )
        copy.start()
        exchanges.append(copy)
    for copy in exchanges:
        copy.wait_recv()
    heights = stats[:, 1]
    tops = heights[:, :, 0:1]
    totals = heights[:, :, 1:2]
    factor = jnp.exp(tops - jnp.max(tops, axis=0, keepdims=True))
    reads = jnp.sum(stats[:, 0] * factor, axis=0) / jnp.sum(totals * factor, axis=0)
    diff = reads - lam_row * pltpu.roll(reads, maps - 1, 0)
    scale = lax.rsqrt(jnp.mean(diff * diff, axis=1, keepdims=True) + 1e-06)
    normed = diff * scale * gain[...]
    headed = jnp.concatenate(
        [
            jnp.broadcast_to(normed[2 * h:2 * h + 1], (MAP_ROWS, wide)).astype(jnp.bfloat16)
            for h in range(heads)
        ],
        axis=1,
    )
    partials = jnp.dot(headed, wo[...], preferred_element_type=jnp.float32)
    partials = partials[:8].astype(jnp.bfloat16).astype(jnp.float32)
    for b in range(n_tp):
        part[b] = partials[:, b * out_cols:(b + 1) * out_cols]
    swaps = []
    for d in range(n_tp - 1, 0, -1):
        target = lax.rem(tp + d, n_tp)
        copy = pltpu.make_async_remote_copy(
            src_ref=part.at[target, pl.ds(0, 1)],
            dst_ref=parts.at[d - 1, pl.ds(0, 1)],
            send_sem=pt_send.at[d - 1],
            recv_sem=pt_recv.at[d - 1],
            device_id={"tp": target},
            device_id_type=MESH,
        )
        copy.start()
        swaps.append(copy)
    mixed = part[tp, 0:1]
    for copy in swaps:
        copy.wait_recv()
    for d in range(1, n_tp):
        mixed = mixed + parts[d - 1, 0:1]
    mix_ref[...] = mixed.astype(jnp.bfloat16)

    near.wait_send()
    for copy in list(far.values()) + list(forwards.values()) + exchanges + swaps:
        copy.wait_send()


def deliver(keys, values, mixed, key_out, value_out, mix_out, sem):
    copies = [
        pltpu.make_async_copy(source, target, sem.at[i])
        for i, (source, target) in enumerate(
            ((keys, key_out), (values, value_out), (mixed, mix_out))
        )
    ]
    for copy in copies:
        copy.start()
    for copy in copies:
        copy.wait()


def tables(length, chunk, head_dim):
    inverse = 1.0 / 10000.0 ** (np.arange(0, head_dim, 2) / head_dim)
    inverse = np.tile(inverse, 4)
    sign = np.tile(np.repeat([-1.0, 1.0], head_dim // 2), 2)

    def pair(positions, axis):
        angles = positions[:, None] * inverse[None, :]
        both = np.stack([np.cos(angles), np.sin(angles) * sign], axis=axis)
        return both.astype(np.float32)

    return pair(np.arange(chunk), 0), pair(np.arange(0, length, chunk), 1)


def on_device(n_sp, n_tp, x, key_weight, value_weight, new_queries, lambdas, head_gain, out_weight):
    heads = lambdas.shape[0]
    columns = key_weight.shape[1]
    head_dim = columns // (2 * heads)
    wide = 2 * head_dim
    seqs, rows, depth = x.shape
    assert seqs == 1
    chunk = rows // 4
    steps = rows // chunk
    chips = n_tp // 2
    pieces = steps - 1 + len(SLICES)
    out_cols = out_weight.shape[1] // n_tp
    fine, coarse = tables(n_sp * n_tp * rows, chunk, head_dim)
    hbm_spec = pl.BlockSpec(memory_space=pltpu.HBM)
    vmem_spec = pl.BlockSpec(memory_space=pltpu.VMEM)
    dma = pltpu.SemaphoreType.DMA
    bf16 = jnp.bfloat16
    f32 = jnp.float32
    room = 2 * n_tp * rows * columns * 2 + SMALL_BYTES
    cache = (n_tp, rows, columns)
    k, v, mixed = pl.pallas_call(
        functools.partial(kernel, n_sp, n_tp, heads, head_dim, chunk),
        out_shape=(
            pltpu.VMEM(cache, bf16),
            pltpu.VMEM(cache, bf16),
            pltpu.VMEM((1, out_cols), bf16),
        ),
        in_specs=[hbm_spec] * 9,
        out_specs=(vmem_spec,) * 3,
        scratch_shapes=[
            pltpu.VMEM((n_tp, rows, depth), bf16),
            pltpu.VMEM((depth, columns), bf16),
            pltpu.VMEM((depth, columns), bf16),
            pltpu.VMEM(out_weight.shape, bf16),
            pltpu.VMEM((1, columns), bf16),
            pltpu.VMEM((1, heads), f32),
            pltpu.VMEM((1, wide), f32),
            pltpu.VMEM((2, chunk, wide), f32),
            pltpu.VMEM((n_tp * steps, 2, wide), f32),
            pltpu.VMEM((n_sp, 2, 2 * heads, wide), f32),
            pltpu.VMEM((n_tp, 8, out_cols), f32),
            pltpu.VMEM((n_tp - 1, 8, out_cols), f32),
            pltpu.VMEM((2 * (chips - 1), chunk, 2 * columns), f32),
            dma((9,)),
            dma((steps,)),
            pltpu.SemaphoreType.REGULAR,
            pltpu.SemaphoreType.REGULAR,
            dma,
            dma,
            dma((chips - 1, pieces)),
            dma((chips - 1, pieces)),
            dma((chips - 1, pieces)),
            dma((chips - 1, pieces)),
            dma((n_sp - 1,)),
            dma((n_sp - 1,)),
            dma((n_tp - 1,)),
            dma((n_tp - 1,)),
        ],
        compiler_params=pltpu.CompilerParams(
            collective_id=0, has_side_effects=True, vmem_limit_bytes=VMEM_BYTES - room
        ),
    )(
        x, key_weight, value_weight, new_queries, lambdas.reshape(1, heads),
        head_gain.reshape(1, wide), out_weight, jnp.asarray(fine), jnp.asarray(coarse),
    )
    k, v, mixed = pl.pallas_call(
        deliver,
        out_shape=(
            jax.ShapeDtypeStruct(cache, bf16),
            jax.ShapeDtypeStruct(cache, bf16),
            jax.ShapeDtypeStruct((1, out_cols), bf16),
        ),
        in_specs=[vmem_spec] * 3,
        out_specs=(hbm_spec,) * 3,
        scratch_shapes=[dma((3,))],
        compiler_params=pltpu.CompilerParams(vmem_limit_bytes=2**20),
    )(k, v, mixed)
    full = (1, n_tp * rows, columns)
    return k.reshape(full), v.reshape(full), mixed


def solution(mesh):
    n_sp, n_tp = mesh.shape["sp"], mesh.shape["tp"]
    in_specs = (
        P("gr", ("sp", "tp"), None),
        P(None, "tp"),
        P(None, "tp"),
        P("gr", "tp"),
        P("tp"),
        P(),
        P("tp", None),
    )
    out_specs = (P("gr", "sp", "tp"), P("gr", "sp", "tp"), P("gr", "tp"))
    return jax.shard_map(
        functools.partial(on_device, n_sp, n_tp),
        mesh=mesh, in_specs=in_specs, out_specs=out_specs, check_vma=False,
    )
```

```python
import functools

import jax
import jax.numpy as jnp
import numpy as np
from jax import lax
from jax.experimental import pallas as pl
from jax.experimental.pallas import tpu as pltpu
from jax.sharding import PartitionSpec as P

MESH = pl.DeviceIdType.MESH
MAP_ROWS = 16
VMEM_BYTES = 67043328
SMALL_BYTES = 16384
SLICES = (3, 2, 2, 1)


def kernel(
    n_sp, n_tp, heads, head_dim, chunk,
    x_ref, wk_ref, wv_ref, q_ref, lam_ref, gain_ref, wo_ref, fine_ref, coarse_ref,
    keys, values, mix_ref,
    xg, wk, wv, wo, q, lam, gain, fine, coarse, stats, part, parts, sums,
    load_sem, own_sem, up_sem, down_sem, near_send, near_recv, far_send, far_recv, fwd_send, fwd_recv,
    st_send, st_recv, pt_send, pt_recv,
):
    sp = lax.axis_index("sp")
    tp = lax.axis_index("tp")
    rows, depth = x_ref.shape[1:]
    columns = wk.shape[1]
    wide = 2 * head_dim
    maps = 2 * heads
    steps = rows // chunk
    chips = n_tp // 2
    partner = tp + 1 - 2 * lax.rem(tp, 2)
    out_cols = mix_ref.shape[1]
    local_coarse = n_tp * steps
    last = steps - 1
    unit = depth // sum(SLICES)
    edges = [unit * sum(SLICES[:i]) for i in range(len(SLICES) + 1)]
    cuts = [slice(edges[i], edges[i + 1]) for i in range(len(SLICES))]
    pieces = [(j, slice(0, depth)) for j in range(last)] + [(last, cut) for cut in cuts]

    def piece_of(block, piece):
        j, cut = pieces[piece]
        return xg.at[block, pl.ds(j * chunk, chunk), pl.ds(cut.start, cut.stop - cut.start)]

    own_loads = [
        pltpu.make_async_copy(
            x_ref.at[0, pl.ds(j * chunk, chunk)], xg.at[tp, pl.ds(j * chunk, chunk)], own_sem.at[j]
        )
        for j in range(steps)
    ]
    loads = [
        pltpu.make_async_copy(q_ref, q, load_sem.at[5]),
        pltpu.make_async_copy(wk_ref, wk, load_sem.at[1]),
        pltpu.make_async_copy(wv_ref, wv, load_sem.at[2]),
        pltpu.make_async_copy(fine_ref, fine, load_sem.at[3]),
        pltpu.make_async_copy(
            coarse_ref.at[pl.ds(sp * local_coarse, local_coarse)], coarse, load_sem.at[4]
        ),
        pltpu.make_async_copy(lam_ref, lam, load_sem.at[6]),
        pltpu.make_async_copy(gain_ref, gain, load_sem.at[7]),
        pltpu.make_async_copy(wo_ref, wo, load_sem.at[8]),
    ]

    barrier = pltpu.get_barrier_semaphore()
    for d in range(1, n_tp):
        pl.semaphore_signal(
            barrier, inc=1, device_id={"tp": lax.rem(tp + d, n_tp)}, device_id_type=MESH
        )
    has_lower = sp > 0
    has_upper = sp < n_sp - 1

    @pl.when(has_lower)
    def _():
        pl.semaphore_signal(barrier, inc=1, device_id={"sp": sp - 1}, device_id_type=MESH)

    @pl.when(has_upper)
    def _():
        pl.semaphore_signal(barrier, inc=1, device_id={"sp": sp + 1}, device_id_type=MESH)

    for load in own_loads:
        load.start()
    pl.semaphore_wait(barrier, n_tp - 1 + jnp.where(has_lower, 1, 0) + jnp.where(has_upper, 1, 0))

    far = {}
    for p in range(len(pieces)):
        if p < steps:
            own_loads[p].wait()
        for d in range(1, chips):
            far[d, p] = pltpu.make_async_remote_copy(
                src_ref=piece_of(tp, p),
                dst_ref=piece_of(tp, p),
                send_sem=far_send.at[d - 1, p],
                recv_sem=far_recv.at[d - 1, p],
                device_id={"tp": lax.rem(partner + 2 * d, n_tp)},
                device_id_type=MESH,
            )
            far[d, p].start()
    near = pltpu.make_async_remote_copy(
        src_ref=xg.at[tp],
        dst_ref=xg.at[tp],
        send_sem=near_send,
        recv_sem=near_recv,
        device_id={"tp": partner},
        device_id_type=MESH,
    )
    near.start()
    for load in loads:
        load.start()

    lane = lax.broadcasted_iota(jnp.int32, (chunk, wide), 1)
    low_half = lax.rem(lane, head_dim) < head_dim // 2

    def settle(block, first, count, raw_keys, raw_values):
        values[block, first * chunk:(first + count) * chunk, :] = raw_values.astype(jnp.bfloat16)
        for i in range(count):
            base = coarse[block * steps + first + i]
            base_cos, base_sin = base[0:1, :], base[1:2, :]
            cosine = base_cos * fine[0] - base_sin * fine[1]
            sine = base_sin * fine[0] + base_cos * fine[1]
            for h in range(heads):
                raw = raw_keys[i * chunk:(i + 1) * chunk, h * wide:(h + 1) * wide]
                ahead = pltpu.roll(raw, wide - head_dim // 2, 1)
                behind = pltpu.roll(raw, head_dim // 2, 1)
                turned = raw * cosine + jnp.where(low_half, ahead, behind) * sine
                keys[
                    block, (first + i) * chunk:(first + i + 1) * chunk, h * wide:(h + 1) * wide
                ] = turned.astype(jnp.bfloat16)

    def product(block, first, count, cut):
        piece = xg[block, first * chunk:(first + count) * chunk, cut]
        raw_keys = jnp.dot(piece, wk[cut, :], preferred_element_type=jnp.float32)
        raw_values = jnp.dot(piece, wv[cut, :], preferred_element_type=jnp.float32)
        return raw_keys, raw_values

    def project(block, first, count):
        settle(block, first, count, *product(block, first, count, slice(0, depth)))

    for load in loads[:5]:
        load.wait()
    map_row = lax.broadcasted_iota(jnp.int32, (MAP_ROWS, columns), 0)
    map_col = lax.broadcasted_iota(jnp.int32, (MAP_ROWS, columns), 1) // head_dim
    spread = jnp.where(map_row == map_col, q[...].astype(jnp.float32), 0.0).astype(jnp.bfloat16)

    def attend(state, block, first, count):
        where = slice(first * chunk, (first + count) * chunk)
        score = lax.dot_general(
            spread, keys[block, where, :], (((1,), (1,)), ((), ())),
            preferred_element_type=jnp.float32,
        ) * head_dim ** (-0.5)
        highest = jnp.max(score, axis=1, keepdims=True)
        if state is not None:
            highest = jnp.maximum(highest, state[0])
        weight = jnp.exp(score - highest)
        total = jnp.sum(weight, axis=1, keepdims=True)
        upper = weight.astype(jnp.bfloat16)
        lower = (weight - upper.astype(jnp.float32)).astype(jnp.bfloat16)
        read = jnp.dot(
            jnp.concatenate([upper, lower], axis=0), values[block, where, :],
            preferred_element_type=jnp.float32,
        )
        read = read[:MAP_ROWS] + read[MAP_ROWS:]
        if state is not None:
            fade = jnp.exp(state[0] - highest)
            total = total + state[1] * fade
            read = read + state[2] * fade
        return highest, total, read

    project(tp, 0, steps)
    state = attend(None, tp, 0, steps)

    pl.when(has_lower)(lambda: pl.semaphore_wait(up_sem, 1))

    @pl.when(has_upper)
    def _():
        pl.semaphore_signal(up_sem, inc=1, device_id={"sp": sp + 1}, device_id_type=MESH)

    near.wait_recv()
    project(partner, 0, steps)
    state = attend(state, partner, 0, steps)

    pl.when(has_upper)(lambda: pl.semaphore_wait(down_sem, 1))

    @pl.when(has_lower)
    def _():
        pl.semaphore_signal(down_sem, inc=1, device_id={"sp": sp - 1}, device_id_type=MESH)

    for load in loads[5:]:
        load.wait()
    map_of = lax.broadcasted_iota(jnp.int32, (maps, wide), 0)
    lam_row = jnp.zeros((maps, wide), jnp.float32)
    for h in range(heads):
        lam_row = jnp.where(map_of == 2 * h, lam[0:1, h:h + 1], lam_row)

    sources = {d: lax.rem(partner + n_tp - 2 * d, n_tp) for d in range(1, chips)}
    others = {d: sources[d] + 1 - 2 * lax.rem(sources[d], 2) for d in sources}
    forwards = {}

    def forward(d, p):
        far[d, p].wait_recv()
        forwards[d, p] = pltpu.make_async_remote_copy(
            src_ref=piece_of(sources[d], p),
            dst_ref=piece_of(sources[d], p),
            send_sem=fwd_send.at[d - 1, p],
            recv_sem=fwd_recv.at[d - 1, p],
            device_id={"tp": partner},
            device_id_type=MESH,
        )
        forwards[d, p].start()

    for j in range(last):
        for d in sources:
            forward(d, j)
            project(sources[d], j, 1)
            state = attend(state, sources[d], j, 1)
            forwards[d, j].wait_recv()
            project(others[d], j, 1)
            state = attend(state, others[d], j, 1)

    def add_slice(d, side, block, i):
        raw_keys, raw_values = product(block, last, 1, cuts[i])
        slot = 2 * (d - 1) + side
        if i > 0:
            raw_keys = raw_keys + sums[slot, :, :columns]
            raw_values = raw_values + sums[slot, :, columns:]
        if i < len(cuts) - 1:
            sums[slot, :, :columns] = raw_keys
            sums[slot, :, columns:] = raw_values
        else:
            settle(block, last, 1, raw_keys, raw_values)

    final = len(cuts) - 1
    for i in range(len(cuts)):
        for d in sources:
            forward(d, last + i)
            if i > 1:
                forwards[d, last + i - 2].wait_recv()
            add_slice(d, 0, sources[d], i)
            if i > 1:
                add_slice(d, 1, others[d], i - 2)
    for d in sources:
        forwards[d, last + final - 1].wait_recv()
        state = attend(state, sources[d], last, 1)
        add_slice(d, 1, others[d], final - 1)
    for d in sources:
        forwards[d, last + final].wait_recv()
        add_slice(d, 1, others[d], final)
        state = attend(state, others[d], last, 1)

    highest, total, read = state
    head_of = lax.broadcasted_iota(jnp.int32, (MAP_ROWS, wide), 0) // 2
    own = jnp.zeros((MAP_ROWS, wide), jnp.float32)
    for h in range(heads):
        own = jnp.where(head_of == h, read[:, h * wide:(h + 1) * wide], own)
    first_lane = lax.broadcasted_iota(jnp.int32, (MAP_ROWS, wide), 1) == 0
    stats[sp, 0] = own[:maps]
    stats[sp, 1] = jnp.where(first_lane, highest, total)[:maps]

    exchanges = []
    for d in range(n_sp - 1, 0, -1):
        copy = pltpu.make_async_remote_copy(
            src_ref=stats.at[sp],
            dst_ref=stats.at[sp],
            send_sem=st_send.at[d - 1],
            recv_sem=st_recv.at[d - 1],
            device_id={"sp": lax.rem(sp + d, n_sp)},
            device_id_type=MESH,
        )
        copy.start()
        exchanges.append(copy)
    for copy in exchanges:
        copy.wait_recv()
    heights = stats[:, 1]
    tops = heights[:, :, 0:1]
    totals = heights[:, :, 1:2]
    factor = jnp.exp(tops - jnp.max(tops, axis=0, keepdims=True))
    reads = jnp.sum(stats[:, 0] * factor, axis=0) / jnp.sum(totals * factor, axis=0)
    diff = reads - lam_row * pltpu.roll(reads, maps - 1, 0)
    scale = lax.rsqrt(jnp.mean(diff * diff, axis=1, keepdims=True) + 1e-06)
    normed = diff * scale * gain[...]
    headed = jnp.concatenate(
        [
            jnp.broadcast_to(normed[2 * h:2 * h + 1], (MAP_ROWS, wide)).astype(jnp.bfloat16)
            for h in range(heads)
        ],
        axis=1,
    )
    partials = jnp.dot(headed, wo[...], preferred_element_type=jnp.float32)
    partials = partials[:8].astype(jnp.bfloat16).astype(jnp.float32)
    for b in range(n_tp):
        part[b] = partials[:, b * out_cols:(b + 1) * out_cols]
    swaps = []
    for d in range(n_tp - 1, 0, -1):
        target = lax.rem(tp + d, n_tp)
        copy = pltpu.make_async_remote_copy(
            src_ref=part.at[target, pl.ds(0, 1)],
            dst_ref=parts.at[d - 1, pl.ds(0, 1)],
            send_sem=pt_send.at[d - 1],
            recv_sem=pt_recv.at[d - 1],
            device_id={"tp": target},
            device_id_type=MESH,
        )
        copy.start()
        swaps.append(copy)
    mixed = part[tp, 0:1]
    for copy in swaps:
        copy.wait_recv()
    for d in range(1, n_tp):
        mixed = mixed + parts[d - 1, 0:1]
    mix_ref[...] = mixed.astype(jnp.bfloat16)

    near.wait_send()
    for copy in list(far.values()) + list(forwards.values()) + exchanges + swaps:
        copy.wait_send()


def deliver(keys, values, mixed, key_out, value_out, mix_out, sem):
    copies = [
        pltpu.make_async_copy(source, target, sem.at[i])
        for i, (source, target) in enumerate(
            ((keys, key_out), (values, value_out), (mixed, mix_out))
        )
    ]
    for copy in copies:
        copy.start()
    for copy in copies:
        copy.wait()


def tables(length, chunk, head_dim):
    inverse = 1.0 / 10000.0 ** (np.arange(0, head_dim, 2) / head_dim)
    inverse = np.tile(inverse, 4)
    sign = np.tile(np.repeat([-1.0, 1.0], head_dim // 2), 2)

    def pair(positions, axis):
        angles = positions[:, None] * inverse[None, :]
        both = np.stack([np.cos(angles), np.sin(angles) * sign], axis=axis)
        return both.astype(np.float32)

    return pair(np.arange(chunk), 0), pair(np.arange(0, length, chunk), 1)


def on_device(n_sp, n_tp, x, key_weight, value_weight, new_queries, lambdas, head_gain, out_weight):
    heads = lambdas.shape[0]
    columns = key_weight.shape[1]
    head_dim = columns // (2 * heads)
    wide = 2 * head_dim
    seqs, rows, depth = x.shape
    assert seqs == 1
    chunk = rows // 4
    steps = rows // chunk
    chips = n_tp // 2
    pieces = steps - 1 + len(SLICES)
    out_cols = out_weight.shape[1] // n_tp
    fine, coarse = tables(n_sp * n_tp * rows, chunk, head_dim)
    hbm_spec = pl.BlockSpec(memory_space=pltpu.HBM)
    vmem_spec = pl.BlockSpec(memory_space=pltpu.VMEM)
    dma = pltpu.SemaphoreType.DMA
    bf16 = jnp.bfloat16
    f32 = jnp.float32
    room = 2 * n_tp * rows * columns * 2 + SMALL_BYTES
    cache = (n_tp, rows, columns)
    k, v, mixed = pl.pallas_call(
        functools.partial(kernel, n_sp, n_tp, heads, head_dim, chunk),
        out_shape=(
            pltpu.VMEM(cache, bf16),
            pltpu.VMEM(cache, bf16),
            pltpu.VMEM((1, out_cols), bf16),
        ),
        in_specs=[hbm_spec] * 9,
        out_specs=(vmem_spec,) * 3,
        scratch_shapes=[
            pltpu.VMEM((n_tp, rows, depth), bf16),
            pltpu.VMEM((depth, columns), bf16),
            pltpu.VMEM((depth, columns), bf16),
            pltpu.VMEM(out_weight.shape, bf16),
            pltpu.VMEM((1, columns), bf16),
            pltpu.VMEM((1, heads), f32),
            pltpu.VMEM((1, wide), f32),
            pltpu.VMEM((2, chunk, wide), f32),
            pltpu.VMEM((n_tp * steps, 2, wide), f32),
            pltpu.VMEM((n_sp, 2, 2 * heads, wide), f32),
            pltpu.VMEM((n_tp, 8, out_cols), f32),
            pltpu.VMEM((n_tp - 1, 8, out_cols), f32),
            pltpu.VMEM((2 * (chips - 1), chunk, 2 * columns), f32),
            dma((9,)),
            dma((steps,)),
            pltpu.SemaphoreType.REGULAR,
            pltpu.SemaphoreType.REGULAR,
            dma,
            dma,
            dma((chips - 1, pieces)),
            dma((chips - 1, pieces)),
            dma((chips - 1, pieces)),
            dma((chips - 1, pieces)),
            dma((n_sp - 1,)),
            dma((n_sp - 1,)),
            dma((n_tp - 1,)),
            dma((n_tp - 1,)),
        ],
        compiler_params=pltpu.CompilerParams(
            collective_id=0, has_side_effects=True, vmem_limit_bytes=VMEM_BYTES - room
        ),
    )(
        x, key_weight, value_weight, new_queries, lambdas.reshape(1, heads),
        head_gain.reshape(1, wide), out_weight, jnp.asarray(fine), jnp.asarray(coarse),
    )
    k, v, mixed = pl.pallas_call(
        deliver,
        out_shape=(
            jax.ShapeDtypeStruct(cache, bf16),
            jax.ShapeDtypeStruct(cache, bf16),
            jax.ShapeDtypeStruct((1, out_cols), bf16),
        ),
        in_specs=[vmem_spec] * 3,
        out_specs=(hbm_spec,) * 3,
        scratch_shapes=[dma((3,))],
        compiler_params=pltpu.CompilerParams(vmem_limit_bytes=2**20),
    )(k, v, mixed)
    full = (1, n_tp * rows, columns)
    return k.reshape(full), v.reshape(full), mixed


def solution(mesh):
    n_sp, n_tp = mesh.shape["sp"], mesh.shape["tp"]
    in_specs = (
        P("gr", ("sp", "tp"), None),
        P(None, "tp"),
        P(None, "tp"),
        P("gr", "tp"),
        P("tp"),
        P(),
        P("tp", None),
    )
    out_specs = (P("gr", "sp", "tp"), P("gr", "sp", "tp"), P("gr", "tp"))
    return jax.shard_map(
        functools.partial(on_device, n_sp, n_tp),
        mesh=mesh, in_specs=in_specs, out_specs=out_specs, check_vma=False,
    )
```

```python
import functools

import jax
import jax.numpy as jnp
import numpy as np
from jax import lax
from jax.experimental import pallas as pl
from jax.experimental.pallas import tpu as pltpu
from jax.sharding import PartitionSpec as P

MESH = pl.DeviceIdType.MESH
MAP_ROWS = 16
VMEM_BYTES = 67043328
SMALL_BYTES = 16384
SLICES = (3, 2, 2, 1)


def kernel(
    n_sp, n_tp, heads, head_dim, chunk,
    x_ref, wk_ref, wv_ref, q_ref, lam_ref, gain_ref, wo_ref, fine_ref, coarse_ref,
    keys, values, mix_ref,
    xg, wk, wv, wo, q, lam, gain, fine, coarse, stats, part, parts, sums,
    load_sem, own_sem, up_sem, down_sem, near_send, near_recv, far_send, far_recv, fwd_send, fwd_recv,
    wo_send, wo_recv, st_send, st_recv, pt_send, pt_recv,
):
    sp = lax.axis_index("sp")
    tp = lax.axis_index("tp")
    rows, depth = x_ref.shape[1:]
    columns = wk.shape[1]
    wide = 2 * head_dim
    maps = 2 * heads
    steps = rows // chunk
    chips = n_tp // 2
    core = lax.rem(tp, 2)
    partner = tp + 1 - 2 * core
    is_lead = core == 1
    out_cols = mix_ref.shape[1]
    local_coarse = n_tp * steps
    last = steps - 1
    unit = depth // sum(SLICES)
    edges = [unit * sum(SLICES[:i]) for i in range(len(SLICES) + 1)]
    cuts = [slice(edges[i], edges[i + 1]) for i in range(len(SLICES))]
    pieces = [(j, slice(0, depth)) for j in range(last)] + [(last, cut) for cut in cuts]

    def piece_of(block, piece):
        j, cut = pieces[piece]
        return xg.at[block, pl.ds(j * chunk, chunk), pl.ds(cut.start, cut.stop - cut.start)]

    own_loads = [
        pltpu.make_async_copy(
            x_ref.at[0, pl.ds(j * chunk, chunk)], xg.at[tp, pl.ds(j * chunk, chunk)], own_sem.at[j]
        )
        for j in range(steps)
    ]
    loads = [
        pltpu.make_async_copy(q_ref, q, load_sem.at[5]),
        pltpu.make_async_copy(wk_ref, wk, load_sem.at[1]),
        pltpu.make_async_copy(wv_ref, wv, load_sem.at[2]),
        pltpu.make_async_copy(fine_ref, fine, load_sem.at[3]),
        pltpu.make_async_copy(
            coarse_ref.at[pl.ds(sp * local_coarse, local_coarse)], coarse, load_sem.at[4]
        ),
        pltpu.make_async_copy(lam_ref, lam, load_sem.at[6]),
        pltpu.make_async_copy(gain_ref, gain, load_sem.at[7]),
    ]
    own_wo = pltpu.make_async_copy(wo_ref, wo.at[pl.ds(columns, columns)], load_sem.at[8])
    lent_wo = pltpu.make_async_remote_copy(
        src_ref=wo_ref,
        dst_ref=wo.at[pl.ds(0, columns)],
        send_sem=wo_send,
        recv_sem=wo_recv,
        device_id={"tp": partner},
        device_id_type=MESH,
    )

    barrier = pltpu.get_barrier_semaphore()
    for d in range(1, n_tp):
        pl.semaphore_signal(
            barrier, inc=1, device_id={"tp": lax.rem(tp + d, n_tp)}, device_id_type=MESH
        )
    has_lower = sp > 0
    has_upper = sp < n_sp - 1

    @pl.when(has_lower)
    def _():
        pl.semaphore_signal(barrier, inc=1, device_id={"sp": sp - 1}, device_id_type=MESH)

    @pl.when(has_upper)
    def _():
        pl.semaphore_signal(barrier, inc=1, device_id={"sp": sp + 1}, device_id_type=MESH)

    for load in own_loads:
        load.start()
    pl.semaphore_wait(barrier, n_tp - 1 + jnp.where(has_lower, 1, 0) + jnp.where(has_upper, 1, 0))

    far = {}
    for p in range(len(pieces)):
        if p < steps:
            own_loads[p].wait()
        for d in range(1, chips):
            far[d, p] = pltpu.make_async_remote_copy(
                src_ref=piece_of(tp, p),
                dst_ref=piece_of(tp, p),
                send_sem=far_send.at[d - 1, p],
                recv_sem=far_recv.at[d - 1, p],
                device_id={"tp": lax.rem(partner + 2 * d, n_tp)},
                device_id_type=MESH,
            )
            far[d, p].start()
    near = pltpu.make_async_remote_copy(
        src_ref=xg.at[tp],
        dst_ref=xg.at[tp],
        send_sem=near_send,
        recv_sem=near_recv,
        device_id={"tp": partner},
        device_id_type=MESH,
    )
    near.start()
    for load in loads:
        load.start()
    pl.when(is_lead)(own_wo.start)
    pl.when(core == 0)(lent_wo.start)

    lane = lax.broadcasted_iota(jnp.int32, (chunk, wide), 1)
    low_half = lax.rem(lane, head_dim) < head_dim // 2

    def settle(block, first, count, raw_keys, raw_values):
        values[block, first * chunk:(first + count) * chunk, :] = raw_values.astype(jnp.bfloat16)
        for i in range(count):
            base = coarse[block * steps + first + i]
            base_cos, base_sin = base[0:1, :], base[1:2, :]
            cosine = base_cos * fine[0] - base_sin * fine[1]
            sine = base_sin * fine[0] + base_cos * fine[1]
            for h in range(heads):
                raw = raw_keys[i * chunk:(i + 1) * chunk, h * wide:(h + 1) * wide]
                ahead = pltpu.roll(raw, wide - head_dim // 2, 1)
                behind = pltpu.roll(raw, head_dim // 2, 1)
                turned = raw * cosine + jnp.where(low_half, ahead, behind) * sine
                keys[
                    block, (first + i) * chunk:(first + i + 1) * chunk, h * wide:(h + 1) * wide
                ] = turned.astype(jnp.bfloat16)

    def product(block, first, count, cut):
        piece = xg[block, first * chunk:(first + count) * chunk, cut]
        raw_keys = jnp.dot(piece, wk[cut, :], preferred_element_type=jnp.float32)
        raw_values = jnp.dot(piece, wv[cut, :], preferred_element_type=jnp.float32)
        return raw_keys, raw_values

    def project(block, first, count):
        settle(block, first, count, *product(block, first, count, slice(0, depth)))

    for load in loads[:5]:
        load.wait()
    map_row = lax.broadcasted_iota(jnp.int32, (MAP_ROWS, columns), 0)
    map_col = lax.broadcasted_iota(jnp.int32, (MAP_ROWS, columns), 1) // head_dim
    spread = jnp.where(map_row == map_col, q[...].astype(jnp.float32), 0.0).astype(jnp.bfloat16)

    def attend(state, block, first, count):
        where = slice(first * chunk, (first + count) * chunk)
        score = lax.dot_general(
            spread, keys[block, where, :], (((1,), (1,)), ((), ())),
            preferred_element_type=jnp.float32,
        ) * head_dim ** (-0.5)
        highest = jnp.max(score, axis=1, keepdims=True)
        if state is not None:
            highest = jnp.maximum(highest, state[0])
        weight = jnp.exp(score - highest)
        total = jnp.sum(weight, axis=1, keepdims=True)
        upper = weight.astype(jnp.bfloat16)
        lower = (weight - upper.astype(jnp.float32)).astype(jnp.bfloat16)
        read = jnp.dot(
            jnp.concatenate([upper, lower], axis=0), values[block, where, :],
            preferred_element_type=jnp.float32,
        )
        read = read[:MAP_ROWS] + read[MAP_ROWS:]
        if state is not None:
            fade = jnp.exp(state[0] - highest)
            total = total + state[1] * fade
            read = read + state[2] * fade
        return highest, total, read

    project(tp, 0, steps)
    state = attend(None, tp, 0, steps)

    pl.when(has_lower)(lambda: pl.semaphore_wait(up_sem, 1))

    @pl.when(has_upper)
    def _():
        pl.semaphore_signal(up_sem, inc=1, device_id={"sp": sp + 1}, device_id_type=MESH)

    near.wait_recv()
    project(partner, 0, steps)
    state = attend(state, partner, 0, steps)

    pl.when(has_upper)(lambda: pl.semaphore_wait(down_sem, 1))

    @pl.when(has_lower)
    def _():
        pl.semaphore_signal(down_sem, inc=1, device_id={"sp": sp - 1}, device_id_type=MESH)

    for load in loads[5:]:
        load.wait()
    map_of = lax.broadcasted_iota(jnp.int32, (maps, wide), 0)
    lam_row = jnp.zeros((maps, wide), jnp.float32)
    for h in range(heads):
        lam_row = jnp.where(map_of == 2 * h, lam[0:1, h:h + 1], lam_row)

    sources = {d: lax.rem(partner + n_tp - 2 * d, n_tp) for d in range(1, chips)}
    others = {d: sources[d] + 1 - 2 * lax.rem(sources[d], 2) for d in sources}
    forwards = {}

    def forward(d, p):
        far[d, p].wait_recv()
        forwards[d, p] = pltpu.make_async_remote_copy(
            src_ref=piece_of(sources[d], p),
            dst_ref=piece_of(sources[d], p),
            send_sem=fwd_send.at[d - 1, p],
            recv_sem=fwd_recv.at[d - 1, p],
            device_id={"tp": partner},
            device_id_type=MESH,
        )
        forwards[d, p].start()

    for j in range(last):
        for d in sources:
            forward(d, j)
            project(sources[d], j, 1)
            state = attend(state, sources[d], j, 1)
            forwards[d, j].wait_recv()
            project(others[d], j, 1)
            state = attend(state, others[d], j, 1)

    def add_slice(d, side, block, i):
        raw_keys, raw_values = product(block, last, 1, cuts[i])
        slot = 2 * (d - 1) + side
        if i > 0:
            raw_keys = raw_keys + sums[slot, :, :columns]
            raw_values = raw_values + sums[slot, :, columns:]
        if i < len(cuts) - 1:
            sums[slot, :, :columns] = raw_keys
            sums[slot, :, columns:] = raw_values
        else:
            settle(block, last, 1, raw_keys, raw_values)

    final = len(cuts) - 1
    for i in range(len(cuts)):
        for d in sources:
            forward(d, last + i)
            if i > 1:
                forwards[d, last + i - 2].wait_recv()
            add_slice(d, 0, sources[d], i)
            if i > 1:
                add_slice(d, 1, others[d], i - 2)
    for d in sources:
        forwards[d, last + final - 1].wait_recv()
        state = attend(state, sources[d], last, 1)
        add_slice(d, 1, others[d], final - 1)
    for d in sources:
        forwards[d, last + final].wait_recv()
        add_slice(d, 1, others[d], final)
        state = attend(state, others[d], last, 1)

    highest, total, read = state
    head_of = lax.broadcasted_iota(jnp.int32, (MAP_ROWS, wide), 0) // 2
    own = jnp.zeros((MAP_ROWS, wide), jnp.float32)
    for h in range(heads):
        own = jnp.where(head_of == h, read[:, h * wide:(h + 1) * wide], own)
    lane_of = lax.broadcasted_iota(jnp.int32, (maps, wide), 1)
    stats[sp, core, 0] = own[:maps]
    stats[sp, core, 1] = jnp.where(
        lane_of == 0, highest[:maps], jnp.where(lane_of == 1, total[:maps], lam_row)
    )

    def stats_copy(d):
        return pltpu.make_async_remote_copy(
            src_ref=stats.at[sp, core],
            dst_ref=stats.at[sp, core],
            send_sem=st_send.at[d],
            recv_sem=st_recv.at[d, core],
            device_id={"sp": lax.rem(sp + d, n_sp), "tp": tp + 1 - core},
            device_id_type=MESH,
        )

    def stats_arrival(d, source):
        return pltpu.make_async_remote_copy(
            src_ref=stats.at[sp, source],
            dst_ref=stats.at[sp, source],
            send_sem=st_send.at[d],
            recv_sem=st_recv.at[d, source],
            device_id={"tp": partner},
            device_id_type=MESH,
        )

    exchanges = [stats_copy(d) for d in range(n_sp - 1, 0, -1)]
    for copy in exchanges:
        copy.start()
    pl.when(core == 0)(stats_copy(0).start)

    def share_copy(d, target):
        chip = lax.rem(tp // 2 + d, chips)
        return pltpu.make_async_remote_copy(
            src_ref=part.at[d, target, pl.ds(0, 1)],
            dst_ref=parts.at[d, pl.ds(0, 1)],
            send_sem=pt_send.at[d, target],
            recv_sem=pt_recv.at[d],
            device_id={"tp": 2 * chip + target},
            device_id_type=MESH,
        )

    @pl.when(is_lead)
    def _():
        own_wo.wait()
        lent_wo.wait_recv()
        stats_arrival(0, 0).wait_recv()
        for d in range(1, n_sp):
            for source in range(2):
                stats_arrival(d, source).wait_recv()
        headed = []
        for c in range(2):
            heights = stats[:, c, 1]
            tops = heights[:, :, 0:1]
            totals = heights[:, :, 1:2]
            factor = jnp.exp(tops - jnp.max(tops, axis=0, keepdims=True))
            reads = jnp.sum(stats[:, c, 0] * factor, axis=0) / jnp.sum(totals * factor, axis=0)
            diff = reads - heights[0, :, 2:3] * pltpu.roll(reads, maps - 1, 0)
            scale = lax.rsqrt(jnp.mean(diff * diff, axis=1, keepdims=True) + 1e-06)
            normed = diff * scale * gain[...]
            row_of = lax.broadcasted_iota(jnp.int32, (MAP_ROWS, wide), 0)
            headed += [
                jnp.where(row_of == c, normed[2 * h:2 * h + 1], 0.0).astype(jnp.bfloat16)
                for h in range(heads)
            ]
        headed = jnp.concatenate(headed, axis=1)
        for d in list(range(1, chips)) + [0]:
            first = pl.multiple_of(lax.rem(tp // 2 + d, chips) * 2 * out_cols, 2 * out_cols)
            partials = jnp.dot(
                headed, wo[:, pl.ds(first, 2 * out_cols)], preferred_element_type=jnp.float32
            )[:8].astype(jnp.bfloat16).astype(jnp.float32)
            both = partials + pltpu.roll(partials, 7, 0)
            for target in range(2):
                part[d, target] = both[:, target * out_cols:(target + 1) * out_cols]
                if d > 0 or target == 0:
                    share_copy(d, target).start()
        mixed = part[0, 1, 0:1]
        for d in range(1, chips):
            share_copy(d, 1).wait_recv()
            mixed = mixed + parts[d, 0:1]
        mix_ref[...] = mixed.astype(jnp.bfloat16)
        for d in range(chips):
            for target in range(2):
                if d > 0 or target == 0:
                    share_copy(d, target).wait_send()

    @pl.when(core == 0)
    def _():
        mixed = None
        for d in range(chips):
            share_copy(d, 1).wait_recv()
            mixed = parts[d, 0:1] if mixed is None else mixed + parts[d, 0:1]
        mix_ref[...] = mixed.astype(jnp.bfloat16)
        lent_wo.wait_send()
        stats_copy(0).wait_send()

    near.wait_send()
    for copy in list(far.values()) + list(forwards.values()) + exchanges:
        copy.wait_send()


def deliver(keys, values, mixed, key_out, value_out, mix_out, sem):
    copies = [
        pltpu.make_async_copy(source, target, sem.at[i])
        for i, (source, target) in enumerate(
            ((keys, key_out), (values, value_out), (mixed, mix_out))
        )
    ]
    for copy in copies:
        copy.start()
    for copy in copies:
        copy.wait()


def tables(length, chunk, head_dim):
    inverse = 1.0 / 10000.0 ** (np.arange(0, head_dim, 2) / head_dim)
    inverse = np.tile(inverse, 4)
    sign = np.tile(np.repeat([-1.0, 1.0], head_dim // 2), 2)

    def pair(positions, axis):
        angles = positions[:, None] * inverse[None, :]
        both = np.stack([np.cos(angles), np.sin(angles) * sign], axis=axis)
        return both.astype(np.float32)

    return pair(np.arange(chunk), 0), pair(np.arange(0, length, chunk), 1)


def on_device(n_sp, n_tp, x, key_weight, value_weight, new_queries, lambdas, head_gain, out_weight):
    heads = lambdas.shape[0]
    columns = key_weight.shape[1]
    head_dim = columns // (2 * heads)
    wide = 2 * head_dim
    seqs, rows, depth = x.shape
    assert seqs == 1
    chunk = rows // 4
    steps = rows // chunk
    chips = n_tp // 2
    pieces = steps - 1 + len(SLICES)
    out_cols = out_weight.shape[1] // n_tp
    fine, coarse = tables(n_sp * n_tp * rows, chunk, head_dim)
    hbm_spec = pl.BlockSpec(memory_space=pltpu.HBM)
    vmem_spec = pl.BlockSpec(memory_space=pltpu.VMEM)
    dma = pltpu.SemaphoreType.DMA
    bf16 = jnp.bfloat16
    f32 = jnp.float32
    room = 2 * n_tp * rows * columns * 2 + SMALL_BYTES
    cache = (n_tp, rows, columns)
    k, v, mixed = pl.pallas_call(
        functools.partial(kernel, n_sp, n_tp, heads, head_dim, chunk),
        out_shape=(
            pltpu.VMEM(cache, bf16),
            pltpu.VMEM(cache, bf16),
            pltpu.VMEM((1, out_cols), bf16),
        ),
        in_specs=[hbm_spec] * 9,
        out_specs=(vmem_spec,) * 3,
        scratch_shapes=[
            pltpu.VMEM((n_tp, rows, depth), bf16),
            pltpu.VMEM((depth, columns), bf16),
            pltpu.VMEM((depth, columns), bf16),
            pltpu.VMEM((2 * columns, out_weight.shape[1]), bf16),
            pltpu.VMEM((1, columns), bf16),
            pltpu.VMEM((1, heads), f32),
            pltpu.VMEM((1, wide), f32),
            pltpu.VMEM((2, chunk, wide), f32),
            pltpu.VMEM((n_tp * steps, 2, wide), f32),
            pltpu.VMEM((n_sp, 2, 2, 2 * heads, wide), f32),
            pltpu.VMEM((chips, 2, 8, out_cols), f32),
            pltpu.VMEM((chips, 8, out_cols), f32),
            pltpu.VMEM((2 * (chips - 1), chunk, 2 * columns), f32),
            dma((9,)),
            dma((steps,)),
            pltpu.SemaphoreType.REGULAR,
            pltpu.SemaphoreType.REGULAR,
            dma,
            dma,
            dma((chips - 1, pieces)),
            dma((chips - 1, pieces)),
            dma((chips - 1, pieces)),
            dma((chips - 1, pieces)),
            dma,
            dma,
            dma((n_sp,)),
            dma((n_sp, 2)),
            dma((chips, 2)),
            dma((chips,)),
        ],
        compiler_params=pltpu.CompilerParams(
            collective_id=0, has_side_effects=True, vmem_limit_bytes=VMEM_BYTES - room
        ),
    )(
        x, key_weight, value_weight, new_queries, lambdas.reshape(1, heads),
        head_gain.reshape(1, wide), out_weight, jnp.asarray(fine), jnp.asarray(coarse),
    )
    k, v, mixed = pl.pallas_call(
        deliver,
        out_shape=(
            jax.ShapeDtypeStruct(cache, bf16),
            jax.ShapeDtypeStruct(cache, bf16),
            jax.ShapeDtypeStruct((1, out_cols), bf16),
        ),
        in_specs=[vmem_spec] * 3,
        out_specs=(hbm_spec,) * 3,
        scratch_shapes=[dma((3,))],
        compiler_params=pltpu.CompilerParams(vmem_limit_bytes=2**20),
    )(k, v, mixed)
    full = (1, n_tp * rows, columns)
    return k.reshape(full), v.reshape(full), mixed


def solution(mesh):
    n_sp, n_tp = mesh.shape["sp"], mesh.shape["tp"]
    in_specs = (
        P("gr", ("sp", "tp"), None),
        P(None, "tp"),
        P(None, "tp"),
        P("gr", "tp"),
        P("tp"),
        P(),
        P("tp", None),
    )
    out_specs = (P("gr", "sp", "tp"), P("gr", "sp", "tp"), P("gr", "tp"))
    return jax.shard_map(
        functools.partial(on_device, n_sp, n_tp),
        mesh=mesh, in_specs=in_specs, out_specs=out_specs, check_vma=False,
    )
```

```python
import functools

import jax
import jax.numpy as jnp
import numpy as np
from jax import lax
from jax.experimental import pallas as pl
from jax.experimental.pallas import tpu as pltpu
from jax.sharding import PartitionSpec as P

MESH = pl.DeviceIdType.MESH
MAP_ROWS = 16
VMEM_BYTES = 67043328
SMALL_BYTES = 16384
SLICES = (3, 2, 2, 1)


def kernel(
    n_sp, n_tp, heads, head_dim, chunk,
    x_ref, wk_ref, wv_ref, q_ref, lam_ref, gain_ref, wo_ref, fine_ref, coarse_ref,
    keys, values, mix_ref,
    xg, wk, wv, wo, q, lam, gain, fine, coarse, stats, part, parts, sums,
    load_sem, own_sem, up_sem, down_sem, near_send, near_recv, far_send, far_recv, twin_send, twin_recv,
    fwd_send, fwd_recv,
    wo_send, wo_recv, st_send, st_recv, pt_send, pt_recv,
):
    sp = lax.axis_index("sp")
    tp = lax.axis_index("tp")
    rows, depth = x_ref.shape[1:]
    columns = wk.shape[1]
    wide = 2 * head_dim
    maps = 2 * heads
    steps = rows // chunk
    chips = n_tp // 2
    core = lax.rem(tp, 2)
    partner = tp + 1 - 2 * core
    is_lead = core == 1
    out_cols = mix_ref.shape[1]
    local_coarse = n_tp * steps
    last = steps - 1
    unit = depth // sum(SLICES)
    edges = [unit * sum(SLICES[:i]) for i in range(len(SLICES) + 1)]
    cuts = [slice(edges[i], edges[i + 1]) for i in range(len(SLICES))]
    pieces = [(j, slice(0, depth)) for j in range(last)] + [(last, cut) for cut in cuts]

    def piece_of(block, piece):
        j, cut = pieces[piece]
        return xg.at[block, pl.ds(j * chunk, chunk), pl.ds(cut.start, cut.stop - cut.start)]

    own_loads = [
        pltpu.make_async_copy(
            x_ref.at[0, pl.ds(j * chunk, chunk)], xg.at[tp, pl.ds(j * chunk, chunk)], own_sem.at[j]
        )
        for j in range(steps)
    ]
    loads = [
        pltpu.make_async_copy(q_ref, q, load_sem.at[5]),
        pltpu.make_async_copy(wk_ref, wk, load_sem.at[1]),
        pltpu.make_async_copy(wv_ref, wv, load_sem.at[2]),
        pltpu.make_async_copy(fine_ref, fine, load_sem.at[3]),
        pltpu.make_async_copy(
            coarse_ref.at[pl.ds(sp * local_coarse, local_coarse)], coarse, load_sem.at[4]
        ),
        pltpu.make_async_copy(lam_ref, lam, load_sem.at[6]),
        pltpu.make_async_copy(gain_ref, gain, load_sem.at[7]),
    ]
    own_wo = pltpu.make_async_copy(wo_ref, wo.at[pl.ds(columns, columns)], load_sem.at[8])
    lent_wo = pltpu.make_async_remote_copy(
        src_ref=wo_ref,
        dst_ref=wo.at[pl.ds(0, columns)],
        send_sem=wo_send,
        recv_sem=wo_recv,
        device_id={"tp": partner},
        device_id_type=MESH,
    )

    barrier = pltpu.get_barrier_semaphore()
    for d in range(1, n_tp):
        pl.semaphore_signal(
            barrier, inc=1, device_id={"tp": lax.rem(tp + d, n_tp)}, device_id_type=MESH
        )
    has_lower = sp > 0
    has_upper = sp < n_sp - 1

    @pl.when(has_lower)
    def _():
        pl.semaphore_signal(barrier, inc=1, device_id={"sp": sp - 1}, device_id_type=MESH)

    @pl.when(has_upper)
    def _():
        pl.semaphore_signal(barrier, inc=1, device_id={"sp": sp + 1}, device_id_type=MESH)

    for load in own_loads:
        load.start()
    pl.semaphore_wait(barrier, n_tp - 1 + jnp.where(has_lower, 1, 0) + jnp.where(has_upper, 1, 0))

    far = {}
    for p in range(len(pieces) - 1):
        if p < steps:
            own_loads[p].wait()
        for d in range(1, chips):
            far[d, p] = pltpu.make_async_remote_copy(
                src_ref=piece_of(tp, p),
                dst_ref=piece_of(tp, p),
                send_sem=far_send.at[d - 1, p],
                recv_sem=far_recv.at[d - 1, p],
                device_id={"tp": lax.rem(partner + 2 * d, n_tp)},
                device_id_type=MESH,
            )
            far[d, p].start()
    twins = {}
    for d in range(1, chips):
        for target in range(2):
            twins[d, target] = pltpu.make_async_remote_copy(
                src_ref=piece_of(tp, len(pieces) - 1),
                dst_ref=piece_of(tp, len(pieces) - 1),
                send_sem=twin_send.at[d - 1, target],
                recv_sem=twin_recv.at[d - 1, core],
                device_id={"tp": lax.rem(tp - core + 2 * d, n_tp) + target},
                device_id_type=MESH,
            )
            twins[d, target].start()
    near = pltpu.make_async_remote_copy(
        src_ref=xg.at[tp],
        dst_ref=xg.at[tp],
        send_sem=near_send,
        recv_sem=near_recv,
        device_id={"tp": partner},
        device_id_type=MESH,
    )
    near.start()
    for load in loads:
        load.start()
    pl.when(is_lead)(own_wo.start)
    pl.when(core == 0)(lent_wo.start)

    lane = lax.broadcasted_iota(jnp.int32, (chunk, wide), 1)
    low_half = lax.rem(lane, head_dim) < head_dim // 2

    def settle(block, first, count, raw_keys, raw_values):
        values[block, first * chunk:(first + count) * chunk, :] = raw_values.astype(jnp.bfloat16)
        for i in range(count):
            base = coarse[block * steps + first + i]
            base_cos, base_sin = base[0:1, :], base[1:2, :]
            cosine = base_cos * fine[0] - base_sin * fine[1]
            sine = base_sin * fine[0] + base_cos * fine[1]
            for h in range(heads):
                raw = raw_keys[i * chunk:(i + 1) * chunk, h * wide:(h + 1) * wide]
                ahead = pltpu.roll(raw, wide - head_dim // 2, 1)
                behind = pltpu.roll(raw, head_dim // 2, 1)
                turned = raw * cosine + jnp.where(low_half, ahead, behind) * sine
                keys[
                    block, (first + i) * chunk:(first + i + 1) * chunk, h * wide:(h + 1) * wide
                ] = turned.astype(jnp.bfloat16)

    def product(block, first, count, cut):
        piece = xg[block, first * chunk:(first + count) * chunk, cut]
        raw_keys = jnp.dot(piece, wk[cut, :], preferred_element_type=jnp.float32)
        raw_values = jnp.dot(piece, wv[cut, :], preferred_element_type=jnp.float32)
        return raw_keys, raw_values

    def project(block, first, count):
        settle(block, first, count, *product(block, first, count, slice(0, depth)))

    for load in loads[:5]:
        load.wait()
    map_row = lax.broadcasted_iota(jnp.int32, (MAP_ROWS, columns), 0)
    map_col = lax.broadcasted_iota(jnp.int32, (MAP_ROWS, columns), 1) // head_dim
    spread = jnp.where(map_row == map_col, q[...].astype(jnp.float32), 0.0).astype(jnp.bfloat16)

    def attend(state, blocks, first, count):
        where = slice(first * chunk, (first + count) * chunk)
        scores = [
            lax.dot_general(
                spread, keys[block, where, :], (((1,), (1,)), ((), ())),
                preferred_element_type=jnp.float32,
            ) * head_dim ** (-0.5)
            for block in blocks
        ]
        highest = functools.reduce(
            jnp.maximum, [jnp.max(score, axis=1, keepdims=True) for score in scores]
        )
        if state is not None:
            highest = jnp.maximum(highest, state[0])
        total, read = 0.0, 0.0
        for block, score in zip(blocks, scores):
            weight = jnp.exp(score - highest)
            total = total + jnp.sum(weight, axis=1, keepdims=True)
            upper = weight.astype(jnp.bfloat16)
            lower = (weight - upper.astype(jnp.float32)).astype(jnp.bfloat16)
            both = jnp.dot(
                jnp.concatenate([upper, lower], axis=0), values[block, where, :],
                preferred_element_type=jnp.float32,
            )
            read = read + both[:MAP_ROWS] + both[MAP_ROWS:]
        if state is not None:
            fade = jnp.exp(state[0] - highest)
            total = total + state[1] * fade
            read = read + state[2] * fade
        return highest, total, read

    project(tp, 0, steps)
    state = attend(None, [tp], 0, steps)

    pl.when(has_lower)(lambda: pl.semaphore_wait(up_sem, 1))

    @pl.when(has_upper)
    def _():
        pl.semaphore_signal(up_sem, inc=1, device_id={"sp": sp + 1}, device_id_type=MESH)

    near.wait_recv()
    project(partner, 0, steps)
    state = attend(state, [partner], 0, steps)

    pl.when(has_upper)(lambda: pl.semaphore_wait(down_sem, 1))

    @pl.when(has_lower)
    def _():
        pl.semaphore_signal(down_sem, inc=1, device_id={"sp": sp - 1}, device_id_type=MESH)

    for load in loads[5:]:
        load.wait()
    map_of = lax.broadcasted_iota(jnp.int32, (maps, wide), 0)
    lam_row = jnp.zeros((maps, wide), jnp.float32)
    for h in range(heads):
        lam_row = jnp.where(map_of == 2 * h, lam[0:1, h:h + 1], lam_row)

    sources = {d: lax.rem(partner + n_tp - 2 * d, n_tp) for d in range(1, chips)}
    others = {d: sources[d] + 1 - 2 * lax.rem(sources[d], 2) for d in sources}
    forwards = {}

    def forward(d, p):
        far[d, p].wait_recv()
        forwards[d, p] = pltpu.make_async_remote_copy(
            src_ref=piece_of(sources[d], p),
            dst_ref=piece_of(sources[d], p),
            send_sem=fwd_send.at[d - 1, p],
            recv_sem=fwd_recv.at[d - 1, p],
            device_id={"tp": partner},
            device_id_type=MESH,
        )
        forwards[d, p].start()

    for j in range(last):
        for d in sources:
            forward(d, j)
            project(sources[d], j, 1)
            state = attend(state, [sources[d]], j, 1)
            forwards[d, j].wait_recv()
            project(others[d], j, 1)
            state = attend(state, [others[d]], j, 1)

    def add_slice(d, side, block, i):
        raw_keys, raw_values = product(block, last, 1, cuts[i])
        slot = 2 * (d - 1) + side
        if i > 0:
            raw_keys = raw_keys + sums[slot, :, :columns]
            raw_values = raw_values + sums[slot, :, columns:]
        sums[slot, :, :columns] = raw_keys
        sums[slot, :, columns:] = raw_values

    final = len(cuts) - 1
    for i in range(final):
        for d in sources:
            forward(d, last + i)
            if i > 1:
                forwards[d, last + i - 2].wait_recv()
            add_slice(d, 0, sources[d], i)
            if i > 1:
                add_slice(d, 1, others[d], i - 2)
    for i in range(max(final - 2, 0), final):
        for d in sources:
            forwards[d, last + i].wait_recv()
            add_slice(d, 1, others[d], i)
    for d in sources:
        pair = (sources[d], others[d])
        for source in range(2):
            pltpu.make_async_remote_copy(
                src_ref=piece_of(sources[d], len(pieces) - 1),
                dst_ref=piece_of(sources[d], len(pieces) - 1),
                send_sem=twin_send.at[d - 1, source],
                recv_sem=twin_recv.at[d - 1, source],
                device_id={"tp": partner},
                device_id_type=MESH,
            ).wait_recv()
        piece = jnp.concatenate(
            [xg[block, last * chunk:rows, cuts[final]] for block in pair], axis=0
        )
        raw_keys = jnp.dot(piece, wk[cuts[final], :], preferred_element_type=jnp.float32)
        raw_values = jnp.dot(piece, wv[cuts[final], :], preferred_element_type=jnp.float32)
        for side, block in enumerate(pair):
            slot = 2 * (d - 1) + side
            part_of = slice(side * chunk, (side + 1) * chunk)
            settle(
                block, last, 1,
                raw_keys[part_of] + sums[slot, :, :columns],
                raw_values[part_of] + sums[slot, :, columns:],
            )
        state = attend(state, pair, last, 1)

    highest, total, read = state
    head_of = lax.broadcasted_iota(jnp.int32, (MAP_ROWS, wide), 0) // 2
    own = jnp.zeros((MAP_ROWS, wide), jnp.float32)
    for h in range(heads):
        own = jnp.where(head_of == h, read[:, h * wide:(h + 1) * wide], own)
    lane_of = lax.broadcasted_iota(jnp.int32, (maps, wide), 1)
    stats[sp, core, 0] = own[:maps]
    stats[sp, core, 1] = jnp.where(
        lane_of == 0, highest[:maps], jnp.where(lane_of == 1, total[:maps], lam_row)
    )

    def stats_copy(target):
        d = lax.rem(target + n_sp - sp, n_sp)
        return pltpu.make_async_remote_copy(
            src_ref=stats.at[sp, core],
            dst_ref=stats.at[sp, core],
            send_sem=st_send.at[d],
            recv_sem=st_recv.at[d, core],
            device_id={"sp": target, "tp": tp + 1 - core},
            device_id_type=MESH,
        )

    def stats_arrival(d, source):
        return pltpu.make_async_remote_copy(
            src_ref=stats.at[sp, source],
            dst_ref=stats.at[sp, source],
            send_sem=st_send.at[d],
            recv_sem=st_recv.at[d, source],
            device_id={"tp": partner},
            device_id_type=MESH,
        )

    exchanges = []
    for k in range(n_sp - 1):
        up, down = k + jnp.where(k >= sp, 1, 0), n_sp - 1 - k - jnp.where(n_sp - 1 - k <= sp, 1, 0)
        exchanges.append(stats_copy(jnp.where(2 * sp >= n_sp, up, down)))
        exchanges[-1].start()
    pl.when(core == 0)(stats_copy(sp).start)

    def share_copy(d, target):
        chip = lax.rem(tp // 2 + d, chips)
        return pltpu.make_async_remote_copy(
            src_ref=part.at[d, target, pl.ds(0, 1)],
            dst_ref=parts.at[d, pl.ds(0, 1)],
            send_sem=pt_send.at[d, target],
            recv_sem=pt_recv.at[d],
            device_id={"tp": 2 * chip + target},
            device_id_type=MESH,
        )

    @pl.when(is_lead)
    def _():
        own_wo.wait()
        lent_wo.wait_recv()
        stats_arrival(0, 0).wait_recv()
        for d in range(1, n_sp):
            for source in range(2):
                stats_arrival(d, source).wait_recv()
        headed, scales = [], []
        row_of = lax.broadcasted_iota(jnp.int32, (2 * MAP_ROWS, wide), 0)
        for c in range(2):
            heights = stats[:, c, 1]
            tops = heights[:, :, 0:1]
            totals = heights[:, :, 1:2]
            factor = jnp.exp(tops - jnp.max(tops, axis=0, keepdims=True))
            reads = jnp.sum(stats[:, c, 0] * factor, axis=0) / jnp.sum(totals * factor, axis=0)
            diff = reads - heights[0, :, 2:3] * pltpu.roll(reads, maps - 1, 0)
            scales.append(lax.rsqrt(jnp.mean(diff * diff, axis=1, keepdims=True) + 1e-06))
            gained = diff * gain[...]
            headed += [
                jnp.where(
                    row_of == c * MAP_ROWS + h, gained[2 * h:2 * h + 1], 0.0
                ).astype(jnp.bfloat16)
                for h in range(heads)
            ]
        headed = jnp.concatenate(headed, axis=1)
        for d in list(range(1, chips)) + [0]:
            for target in range(2):
                column = (2 * lax.rem(tp // 2 + d, chips) + target) * out_cols
                first = pl.multiple_of(column, out_cols)
                shares = jnp.dot(
                    headed, wo[:, pl.ds(first, out_cols)], preferred_element_type=jnp.float32
                )
                both = 0.0
                for c in range(2):
                    group = 0.0
                    for h in range(heads):
                        row = c * MAP_ROWS + h
                        group = group + shares[row:row + 1] * scales[c][2 * h:2 * h + 1]
                    both = both + group.astype(jnp.bfloat16).astype(jnp.float32)
                part[d, target, 0:1] = both
                if d > 0 or target == 0:
                    share_copy(d, target).start()
        mixed = part[0, 1, 0:1]
        for d in range(1, chips):
            share_copy(d, 1).wait_recv()
            mixed = mixed + parts[d, 0:1]
        mix_ref[...] = mixed.astype(jnp.bfloat16)
        for d in range(chips):
            for target in range(2):
                if d > 0 or target == 0:
                    share_copy(d, target).wait_send()

    @pl.when(core == 0)
    def _():
        mixed = None
        for d in range(chips):
            share_copy(d, 1).wait_recv()
            mixed = parts[d, 0:1] if mixed is None else mixed + parts[d, 0:1]
        mix_ref[...] = mixed.astype(jnp.bfloat16)
        lent_wo.wait_send()
        stats_copy(sp).wait_send()

    near.wait_send()
    for copy in [*far.values(), *twins.values(), *forwards.values(), *exchanges]:
        copy.wait_send()


def deliver(keys, values, mixed, key_out, value_out, mix_out, sem):
    copies = [
        pltpu.make_async_copy(source, target, sem.at[i])
        for i, (source, target) in enumerate(
            ((keys, key_out), (values, value_out), (mixed, mix_out))
        )
    ]
    for copy in copies:
        copy.start()
    for copy in copies:
        copy.wait()


def tables(length, chunk, head_dim):
    inverse = 1.0 / 10000.0 ** (np.arange(0, head_dim, 2) / head_dim)
    inverse = np.tile(inverse, 4)
    sign = np.tile(np.repeat([-1.0, 1.0], head_dim // 2), 2)

    def pair(positions, axis):
        angles = positions[:, None] * inverse[None, :]
        both = np.stack([np.cos(angles), np.sin(angles) * sign], axis=axis)
        return both.astype(np.float32)

    return pair(np.arange(chunk), 0), pair(np.arange(0, length, chunk), 1)


def on_device(n_sp, n_tp, x, key_weight, value_weight, new_queries, lambdas, head_gain, out_weight):
    heads = lambdas.shape[0]
    columns = key_weight.shape[1]
    head_dim = columns // (2 * heads)
    wide = 2 * head_dim
    seqs, rows, depth = x.shape
    assert seqs == 1
    chunk = rows // 4
    steps = rows // chunk
    chips = n_tp // 2
    pieces = steps - 1 + len(SLICES)
    out_cols = out_weight.shape[1] // n_tp
    fine, coarse = tables(n_sp * n_tp * rows, chunk, head_dim)
    hbm_spec = pl.BlockSpec(memory_space=pltpu.HBM)
    vmem_spec = pl.BlockSpec(memory_space=pltpu.VMEM)
    dma = pltpu.SemaphoreType.DMA
    bf16 = jnp.bfloat16
    f32 = jnp.float32
    room = 2 * n_tp * rows * columns * 2 + SMALL_BYTES
    cache = (n_tp, rows, columns)
    k, v, mixed = pl.pallas_call(
        functools.partial(kernel, n_sp, n_tp, heads, head_dim, chunk),
        out_shape=(
            pltpu.VMEM(cache, bf16),
            pltpu.VMEM(cache, bf16),
            pltpu.VMEM((1, out_cols), bf16),
        ),
        in_specs=[hbm_spec] * 9,
        out_specs=(vmem_spec,) * 3,
        scratch_shapes=[
            pltpu.VMEM((n_tp, rows, depth), bf16),
            pltpu.VMEM((depth, columns), bf16),
            pltpu.VMEM((depth, columns), bf16),
            pltpu.VMEM((2 * columns, out_weight.shape[1]), bf16),
            pltpu.VMEM((1, columns), bf16),
            pltpu.VMEM((1, heads), f32),
            pltpu.VMEM((1, wide), f32),
            pltpu.VMEM((2, chunk, wide), f32),
            pltpu.VMEM((n_tp * steps, 2, wide), f32),
            pltpu.VMEM((n_sp, 2, 2, 2 * heads, wide), f32),
            pltpu.VMEM((chips, 2, 8, out_cols), f32),
            pltpu.VMEM((chips, 8, out_cols), f32),
            pltpu.VMEM((2 * (chips - 1), chunk, 2 * columns), f32),
            dma((9,)),
            dma((steps,)),
            pltpu.SemaphoreType.REGULAR,
            pltpu.SemaphoreType.REGULAR,
            dma,
            dma,
            dma((chips - 1, pieces - 1)),
            dma((chips - 1, pieces - 1)),
            dma((chips - 1, 2)),
            dma((chips - 1, 2)),
            dma((chips - 1, pieces - 1)),
            dma((chips - 1, pieces - 1)),
            dma,
            dma,
            dma((n_sp,)),
            dma((n_sp, 2)),
            dma((chips, 2)),
            dma((chips,)),
        ],
        compiler_params=pltpu.CompilerParams(
            collective_id=0, has_side_effects=True, vmem_limit_bytes=VMEM_BYTES - room
        ),
    )(
        x, key_weight, value_weight, new_queries, lambdas.reshape(1, heads),
        head_gain.reshape(1, wide), out_weight, jnp.asarray(fine), jnp.asarray(coarse),
    )
    k, v, mixed = pl.pallas_call(
        deliver,
        out_shape=(
            jax.ShapeDtypeStruct(cache, bf16),
            jax.ShapeDtypeStruct(cache, bf16),
            jax.ShapeDtypeStruct((1, out_cols), bf16),
        ),
        in_specs=[vmem_spec] * 3,
        out_specs=(hbm_spec,) * 3,
        scratch_shapes=[dma((3,))],
        compiler_params=pltpu.CompilerParams(vmem_limit_bytes=2**20),
    )(k, v, mixed)
    full = (1, n_tp * rows, columns)
    return k.reshape(full), v.reshape(full), mixed


def solution(mesh):
    n_sp, n_tp = mesh.shape["sp"], mesh.shape["tp"]
    in_specs = (
        P("gr", ("sp", "tp"), None),
        P(None, "tp"),
        P(None, "tp"),
        P("gr", "tp"),
        P("tp"),
        P(),
        P("tp", None),
    )
    out_specs = (P("gr", "sp", "tp"), P("gr", "sp", "tp"), P("gr", "tp"))
    return jax.shard_map(
        functools.partial(on_device, n_sp, n_tp),
        mesh=mesh, in_specs=in_specs, out_specs=out_specs, check_vma=False,
    )
```

```python
import functools

import jax
import jax.numpy as jnp
import numpy as np
from jax import lax
from jax.experimental import pallas as pl
from jax.experimental.pallas import tpu as pltpu
from jax.sharding import PartitionSpec as P

MESH = pl.DeviceIdType.MESH
MAP_ROWS = 16
LANES = 128
VMEM_BYTES = 67043328
SMALL_BYTES = 16384
SLICES = (5, 2, 1)


def kernel(
    n_sp, n_tp, heads, head_dim, chunk,
    x_ref, wk_ref, wv_ref, q_ref, lam_ref, gain_ref, wo_ref, fine_ref, coarse_ref,
    keys, values, mix_ref,
    xg, wk, wv, wo, q, lam, gain, fine, coarse, stats, part, parts, sums, turned_q, pick,
    load_sem, own_sem, up_sem, down_sem, near_send, near_recv, far_send, far_recv, twin_send, twin_recv,
    fwd_send, fwd_recv,
    wo_send, wo_recv, st_send, st_recv, pt_send, pt_recv,
):
    sp = lax.axis_index("sp")
    tp = lax.axis_index("tp")
    rows, depth = x_ref.shape[1:]
    columns = wk.shape[1]
    wide = 2 * head_dim
    maps = 2 * heads
    steps = rows // chunk
    chips = n_tp // 2
    core = lax.rem(tp, 2)
    partner = tp + 1 - 2 * core
    is_lead = core == 1
    out_cols = mix_ref.shape[1]
    local_coarse = n_tp * steps
    last = steps - 1
    unit = depth // sum(SLICES)
    edges = [unit * sum(SLICES[:i]) for i in range(len(SLICES) + 1)]
    cuts = [slice(edges[i], edges[i + 1]) for i in range(len(SLICES))]
    pieces = [(j, slice(0, depth)) for j in range(last)] + [(last, cut) for cut in cuts]

    def piece_of(block, piece):
        j, cut = pieces[piece]
        return xg.at[block, pl.ds(j * chunk, chunk), pl.ds(cut.start, cut.stop - cut.start)]

    own_loads = [
        pltpu.make_async_copy(
            x_ref.at[0, pl.ds(j * chunk, chunk)], xg.at[tp, pl.ds(j * chunk, chunk)], own_sem.at[j]
        )
        for j in range(steps)
    ]
    loads = [
        pltpu.make_async_copy(q_ref, q, load_sem.at[5]),
        pltpu.make_async_copy(wk_ref, wk, load_sem.at[1]),
        pltpu.make_async_copy(wv_ref, wv, load_sem.at[2]),
        pltpu.make_async_copy(fine_ref, fine, load_sem.at[3]),
        pltpu.make_async_copy(
            coarse_ref.at[pl.ds(sp * local_coarse, local_coarse)], coarse, load_sem.at[4]
        ),
        pltpu.make_async_copy(lam_ref, lam, load_sem.at[6]),
        pltpu.make_async_copy(gain_ref, gain, load_sem.at[7]),
    ]
    own_wo = pltpu.make_async_copy(wo_ref, wo.at[pl.ds(columns, columns)], load_sem.at[8])
    lent_wo = pltpu.make_async_remote_copy(
        src_ref=wo_ref,
        dst_ref=wo.at[pl.ds(0, columns)],
        send_sem=wo_send,
        recv_sem=wo_recv,
        device_id={"tp": partner},
        device_id_type=MESH,
    )

    own_loads[0].start()
    barrier = pltpu.get_barrier_semaphore()
    for d in range(1, n_tp):
        pl.semaphore_signal(
            barrier, inc=1, device_id={"tp": lax.rem(tp + d, n_tp)}, device_id_type=MESH
        )
    has_lower = sp > 0
    has_upper = sp < n_sp - 1

    @pl.when(has_lower)
    def _():
        pl.semaphore_signal(barrier, inc=1, device_id={"sp": sp - 1}, device_id_type=MESH)

    @pl.when(has_upper)
    def _():
        pl.semaphore_signal(barrier, inc=1, device_id={"sp": sp + 1}, device_id_type=MESH)

    for load in own_loads[1:]:
        load.start()
    pl.semaphore_wait(barrier, n_tp - 1 + jnp.where(has_lower, 1, 0) + jnp.where(has_upper, 1, 0))

    far = {}
    for p in range(len(pieces) - 1):
        if p < steps:
            own_loads[p].wait()
        for d in range(1, chips):
            far[d, p] = pltpu.make_async_remote_copy(
                src_ref=piece_of(tp, p),
                dst_ref=piece_of(tp, p),
                send_sem=far_send.at[d - 1, p],
                recv_sem=far_recv.at[d - 1, p],
                device_id={"tp": lax.rem(partner + 2 * d, n_tp)},
                device_id_type=MESH,
            )
            far[d, p].start()
    twins = {}
    for d in range(1, chips):
        for target in range(2):
            twins[d, target] = pltpu.make_async_remote_copy(
                src_ref=piece_of(tp, len(pieces) - 1),
                dst_ref=piece_of(tp, len(pieces) - 1),
                send_sem=twin_send.at[d - 1, target],
                recv_sem=twin_recv.at[d - 1, core],
                device_id={"tp": lax.rem(tp - core + 2 * d, n_tp) + target},
                device_id_type=MESH,
            )
            twins[d, target].start()
    near = pltpu.make_async_remote_copy(
        src_ref=xg.at[tp],
        dst_ref=xg.at[tp],
        send_sem=near_send,
        recv_sem=near_recv,
        device_id={"tp": partner},
        device_id_type=MESH,
    )
    near.start()
    for load in loads:
        load.start()
    pl.when(is_lead)(own_wo.start)
    pl.when(core == 0)(lent_wo.start)

    lane = lax.broadcasted_iota(jnp.int32, (chunk, wide), 1)
    low_half = lax.rem(lane, head_dim) < head_dim // 2

    def angles(block, j):
        base = coarse[block * steps + j]
        base_cos, base_sin = base[0:1, :], base[1:2, :]
        cosine = base_cos * fine[0] - base_sin * fine[1]
        sine = base_sin * fine[0] + base_cos * fine[1]
        return cosine, sine

    def swapped(raw):
        ahead = pltpu.roll(raw, wide - head_dim // 2, 1)
        behind = pltpu.roll(raw, head_dim // 2, 1)
        return jnp.where(low_half, ahead, behind)

    def settle(block, first, count, raw_keys, raw_values):
        values[block, first * chunk:(first + count) * chunk, :] = raw_values.astype(jnp.bfloat16)
        for i in range(count):
            cosine, sine = angles(block, first + i)
            for h in range(heads):
                raw = raw_keys[i * chunk:(i + 1) * chunk, h * wide:(h + 1) * wide]
                turned = raw * cosine + swapped(raw) * sine
                keys[
                    block, (first + i) * chunk:(first + i + 1) * chunk, h * wide:(h + 1) * wide
                ] = turned.astype(jnp.bfloat16)

    def product(block, first, count, cut):
        piece = xg[block, first * chunk:(first + count) * chunk, cut]
        raw_keys = jnp.dot(piece, wk[cut, :], preferred_element_type=jnp.float32)
        raw_values = jnp.dot(piece, wv[cut, :], preferred_element_type=jnp.float32)
        return raw_keys, raw_values

    def project(block, first, count):
        settle(block, first, count, *product(block, first, count, slice(0, depth)))

    for load in loads[:5]:
        load.wait()
    map_row = lax.broadcasted_iota(jnp.int32, (MAP_ROWS, columns), 0)
    map_col = lax.broadcasted_iota(jnp.int32, (MAP_ROWS, columns), 1) // head_dim
    spread = jnp.where(map_row == map_col, q[...].astype(jnp.float32), 0.0).astype(jnp.bfloat16)

    def weigh(highest, weight, rows_of_values):
        total = jnp.sum(weight, axis=1, keepdims=True)
        upper = weight.astype(jnp.bfloat16)
        lower = (weight - upper.astype(jnp.float32)).astype(jnp.bfloat16)
        read = jnp.dot(
            jnp.concatenate([upper, lower], axis=0), rows_of_values,
            preferred_element_type=jnp.float32,
        )
        return highest, total, read[:MAP_ROWS] + read[MAP_ROWS:]

    def merge(one, two):
        highest = jnp.maximum(one[0], two[0])
        fades = jnp.exp(one[0] - highest), jnp.exp(two[0] - highest)
        return (
            highest,
            one[1] * fades[0] + two[1] * fades[1],
            one[2] * fades[0] + two[2] * fades[1],
        )

    def attend(state, block, first, count):
        where = slice(first * chunk, (first + count) * chunk)
        score = lax.dot_general(
            spread, keys[block, where, :], (((1,), (1,)), ((), ())),
            preferred_element_type=jnp.float32,
        ) * head_dim ** (-0.5)
        highest = jnp.max(score, axis=1, keepdims=True)
        fresh = weigh(highest, jnp.exp(score - highest), values[block, where, :])
        return fresh if state is None else merge(state, fresh)

    def attend_raw(state, slots, raw_keys, raw_values):
        products = jnp.concatenate(
            [raw * turned_q[slot] for raw, slot in zip(raw_keys, slots)], axis=0
        )
        count = products.shape[0]
        upper = products.astype(jnp.bfloat16)
        lower = (products - upper.astype(jnp.float32)).astype(jnp.bfloat16)
        score = jnp.dot(
            jnp.concatenate([upper, lower], axis=0), pick[...], preferred_element_type=jnp.float32
        )
        score = score[:count] + score[count:]
        highest = jnp.max(score, axis=0, keepdims=True)
        room = -(-(count + 8) // LANES) * LANES - count
        across = jnp.transpose(
            jnp.concatenate(
                [jnp.exp(score - highest), jnp.broadcast_to(highest, (room, LANES))], axis=0
            )
        )[:MAP_ROWS]
        rows_of_values = jnp.concatenate(raw_values, axis=0).astype(jnp.bfloat16)
        fresh = weigh(across[:, count:count + 1], across[:, :count], rows_of_values)
        return merge(state, fresh)

    project(tp, 0, steps)
    state = attend(None, tp, 0, steps)

    pl.when(has_lower)(lambda: pl.semaphore_wait(up_sem, 1))

    @pl.when(has_upper)
    def _():
        pl.semaphore_signal(up_sem, inc=1, device_id={"sp": sp + 1}, device_id_type=MESH)

    near.wait_recv()
    project(partner, 0, steps)
    state = attend(state, partner, 0, steps)

    pl.when(has_upper)(lambda: pl.semaphore_wait(down_sem, 1))

    @pl.when(has_lower)
    def _():
        pl.semaphore_signal(down_sem, inc=1, device_id={"sp": sp - 1}, device_id_type=MESH)

    for load in loads[5:]:
        load.wait()
    map_of = lax.broadcasted_iota(jnp.int32, (maps, wide), 0)
    lam_row = jnp.zeros((maps, wide), jnp.float32)
    for h in range(heads):
        lam_row = jnp.where(map_of == 2 * h, lam[0:1, h:h + 1], lam_row)

    sources = {d: lax.rem(partner + n_tp - 2 * d, n_tp) for d in range(1, chips)}
    others = {d: sources[d] + 1 - 2 * lax.rem(sources[d], 2) for d in sources}
    forwards = {}

    pick_row = lax.broadcasted_iota(jnp.int32, (columns, LANES), 0) // head_dim
    pick_lane = lax.broadcasted_iota(jnp.int32, (columns, LANES), 1)
    pick[...] = jnp.where(pick_row == pick_lane, 1.0, 0.0).astype(jnp.bfloat16)
    for d in sources:
        for side, block in enumerate((sources[d], others[d])):
            cosine, sine = angles(block, last)
            for h in range(heads):
                query = jnp.broadcast_to(
                    q[0:1, h * wide:(h + 1) * wide].astype(jnp.float32), (chunk, wide)
                )
                turned_q[2 * (d - 1) + side, :, h * wide:(h + 1) * wide] = (
                    query * cosine - swapped(query) * sine
                ) * head_dim ** (-0.5)

    def forward(d, p):
        far[d, p].wait_recv()
        forwards[d, p] = pltpu.make_async_remote_copy(
            src_ref=piece_of(sources[d], p),
            dst_ref=piece_of(sources[d], p),
            send_sem=fwd_send.at[d - 1, p],
            recv_sem=fwd_recv.at[d - 1, p],
            device_id={"tp": partner},
            device_id_type=MESH,
        )
        forwards[d, p].start()

    for j in range(last):
        for d in sources:
            forward(d, j)
            project(sources[d], j, 1)
            state = attend(state, sources[d], j, 1)
            forwards[d, j].wait_recv()
            project(others[d], j, 1)
            state = attend(state, others[d], j, 1)

    tail = slice(edges[1], depth)

    def add_first(slot, block):
        sums[slot, :, :columns], sums[slot, :, columns:] = product(block, last, 1, cuts[0])

    for d in sources:
        forward(d, last)
        add_first(2 * d - 2, sources[d])
    for i in range(1, len(cuts) - 1):
        for d in sources:
            forward(d, last + i)
    for d in sources:
        forwards[d, last].wait_recv()
        add_first(2 * d - 1, others[d])
    for d in sources:
        pair = (sources[d], others[d])
        for i in range(1, len(cuts) - 1):
            forwards[d, last + i].wait_recv()
        for source in range(2):
            pltpu.make_async_remote_copy(
                src_ref=piece_of(sources[d], len(pieces) - 1),
                dst_ref=piece_of(sources[d], len(pieces) - 1),
                send_sem=twin_send.at[d - 1, source],
                recv_sem=twin_recv.at[d - 1, source],
                device_id={"tp": partner},
                device_id_type=MESH,
            ).wait_recv()
        both = jnp.concatenate([xg[block, last * chunk:rows, tail] for block in pair], axis=0)
        raws = []
        for w, where in ((wk, slice(0, columns)), (wv, slice(columns, 2 * columns))):
            raw = jnp.dot(both, w[tail, :], preferred_element_type=jnp.float32)
            raws.append([
                raw[side * chunk:(side + 1) * chunk] + sums[2 * (d - 1) + side, :, where]
                for side in range(2)
            ])
        for side, block in enumerate(pair):
            settle(block, last, 1, raws[0][side], raws[1][side])
        state = attend_raw(state, (2 * d - 2, 2 * d - 1), *raws)

    highest, total, read = state
    head_of = lax.broadcasted_iota(jnp.int32, (MAP_ROWS, wide), 0) // 2
    own = jnp.zeros((MAP_ROWS, wide), jnp.float32)
    for h in range(heads):
        own = jnp.where(head_of == h, read[:, h * wide:(h + 1) * wide], own)
    lane_of = lax.broadcasted_iota(jnp.int32, (maps, wide), 1)
    stats[sp, core, 0] = own[:maps]
    stats[sp, core, 1] = jnp.where(
        lane_of == 0, highest[:maps], jnp.where(lane_of == 1, total[:maps], lam_row)
    )

    def stats_copy(target):
        d = lax.rem(target + n_sp - sp, n_sp)
        return pltpu.make_async_remote_copy(
            src_ref=stats.at[sp, core],
            dst_ref=stats.at[sp, core],
            send_sem=st_send.at[d],
            recv_sem=st_recv.at[d, core],
            device_id={"sp": target, "tp": tp + 1 - core},
            device_id_type=MESH,
        )

    def stats_arrival(d, source):
        return pltpu.make_async_remote_copy(
            src_ref=stats.at[sp, source],
            dst_ref=stats.at[sp, source],
            send_sem=st_send.at[d],
            recv_sem=st_recv.at[d, source],
            device_id={"tp": partner},
            device_id_type=MESH,
        )

    exchanges = []
    for k in range(n_sp - 1):
        up, down = k + jnp.where(k >= sp, 1, 0), n_sp - 1 - k - jnp.where(n_sp - 1 - k <= sp, 1, 0)
        exchanges.append(stats_copy(jnp.where(2 * sp >= n_sp, up, down)))
        exchanges[-1].start()
    pl.when(core == 0)(stats_copy(sp).start)

    def share_copy(d, target):
        chip = lax.rem(tp // 2 + d, chips)
        return pltpu.make_async_remote_copy(
            src_ref=part.at[d, target, pl.ds(0, 1)],
            dst_ref=parts.at[d, pl.ds(0, 1)],
            send_sem=pt_send.at[d, target],
            recv_sem=pt_recv.at[d],
            device_id={"tp": 2 * chip + target},
            device_id_type=MESH,
        )

    @pl.when(is_lead)
    def _():
        own_wo.wait()
        lent_wo.wait_recv()
        stats_arrival(0, 0).wait_recv()
        for d in range(1, n_sp):
            for source in range(2):
                stats_arrival(d, source).wait_recv()
        headed, scales = [], []
        row_of = lax.broadcasted_iota(jnp.int32, (2 * MAP_ROWS, wide), 0)
        for c in range(2):
            heights = stats[:, c, 1]
            tops = heights[:, :, 0:1]
            totals = heights[:, :, 1:2]
            factor = jnp.exp(tops - jnp.max(tops, axis=0, keepdims=True))
            reads = jnp.sum(stats[:, c, 0] * factor, axis=0) / jnp.sum(totals * factor, axis=0)
            diff = reads - heights[0, :, 2:3] * pltpu.roll(reads, maps - 1, 0)
            scales.append(lax.rsqrt(jnp.mean(diff * diff, axis=1, keepdims=True) + 1e-06))
            gained = diff * gain[...]
            headed += [
                jnp.where(
                    row_of == c * MAP_ROWS + h, gained[2 * h:2 * h + 1], 0.0
                ).astype(jnp.bfloat16)
                for h in range(heads)
            ]
        headed = jnp.concatenate(headed, axis=1)
        for d in list(range(1, chips)) + [0]:
            for target in range(2):
                column = (2 * lax.rem(tp // 2 + d, chips) + target) * out_cols
                first = pl.multiple_of(column, out_cols)
                shares = jnp.dot(
                    headed, wo[:, pl.ds(first, out_cols)], preferred_element_type=jnp.float32
                )
                both = 0.0
                for c in range(2):
                    group = 0.0
                    for h in range(heads):
                        row = c * MAP_ROWS + h
                        group = group + shares[row:row + 1] * scales[c][2 * h:2 * h + 1]
                    both = both + group.astype(jnp.bfloat16).astype(jnp.float32)
                part[d, target, 0:1] = both
                if d > 0 or target == 0:
                    share_copy(d, target).start()
        mixed = part[0, 1, 0:1]
        for d in range(1, chips):
            share_copy(d, 1).wait_recv()
            mixed = mixed + parts[d, 0:1]
        mix_ref[...] = mixed.astype(jnp.bfloat16)
        for d in range(chips):
            for target in range(2):
                if d > 0 or target == 0:
                    share_copy(d, target).wait_send()

    @pl.when(core == 0)
    def _():
        mixed = None
        for d in range(chips):
            share_copy(d, 1).wait_recv()
            mixed = parts[d, 0:1] if mixed is None else mixed + parts[d, 0:1]
        mix_ref[...] = mixed.astype(jnp.bfloat16)
        lent_wo.wait_send()
        stats_copy(sp).wait_send()

    near.wait_send()
    for copy in [*far.values(), *twins.values(), *forwards.values(), *exchanges]:
        copy.wait_send()


def deliver(keys, values, mixed, key_out, value_out, mix_out, sem):
    copies = [
        pltpu.make_async_copy(source, target, sem.at[i])
        for i, (source, target) in enumerate(
            ((keys, key_out), (values, value_out), (mixed, mix_out))
        )
    ]
    for copy in copies:
        copy.start()
    for copy in copies:
        copy.wait()


def tables(length, chunk, head_dim):
    inverse = 1.0 / 10000.0 ** (np.arange(0, head_dim, 2) / head_dim)
    inverse = np.tile(inverse, 4)
    sign = np.tile(np.repeat([-1.0, 1.0], head_dim // 2), 2)

    def pair(positions, axis):
        angles = positions[:, None] * inverse[None, :]
        both = np.stack([np.cos(angles), np.sin(angles) * sign], axis=axis)
        return both.astype(np.float32)

    return pair(np.arange(chunk), 0), pair(np.arange(0, length, chunk), 1)


def on_device(n_sp, n_tp, x, key_weight, value_weight, new_queries, lambdas, head_gain, out_weight):
    heads = lambdas.shape[0]
    columns = key_weight.shape[1]
    head_dim = columns // (2 * heads)
    wide = 2 * head_dim
    seqs, rows, depth = x.shape
    assert seqs == 1
    chunk = rows // 4
    steps = rows // chunk
    chips = n_tp // 2
    pieces = steps - 1 + len(SLICES)
    out_cols = out_weight.shape[1] // n_tp
    fine, coarse = tables(n_sp * n_tp * rows, chunk, head_dim)
    hbm_spec = pl.BlockSpec(memory_space=pltpu.HBM)
    vmem_spec = pl.BlockSpec(memory_space=pltpu.VMEM)
    dma = pltpu.SemaphoreType.DMA
    bf16 = jnp.bfloat16
    f32 = jnp.float32
    room = 2 * n_tp * rows * columns * 2 + SMALL_BYTES
    cache = (n_tp, rows, columns)
    k, v, mixed = pl.pallas_call(
        functools.partial(kernel, n_sp, n_tp, heads, head_dim, chunk),
        out_shape=(
            pltpu.VMEM(cache, bf16),
            pltpu.VMEM(cache, bf16),
            pltpu.VMEM((1, out_cols), bf16),
        ),
        in_specs=[hbm_spec] * 9,
        out_specs=(vmem_spec,) * 3,
        scratch_shapes=[
            pltpu.VMEM((n_tp, rows, depth), bf16),
            pltpu.VMEM((depth, columns), bf16),
            pltpu.VMEM((depth, columns), bf16),
            pltpu.VMEM((2 * columns, out_weight.shape[1]), bf16),
            pltpu.VMEM((1, columns), bf16),
            pltpu.VMEM((1, heads), f32),
            pltpu.VMEM((1, wide), f32),
            pltpu.VMEM((2, chunk, wide), f32),
            pltpu.VMEM((n_tp * steps, 2, wide), f32),
            pltpu.VMEM((n_sp, 2, 2, 2 * heads, wide), f32),
            pltpu.VMEM((chips, 2, 8, out_cols), f32),
            pltpu.VMEM((chips, 8, out_cols), f32),
            pltpu.VMEM((2 * (chips - 1), chunk, 2 * columns), f32),
            pltpu.VMEM((2 * (chips - 1), chunk, columns), f32),
            pltpu.VMEM((columns, LANES), bf16),
            dma((9,)),
            dma((steps,)),
            pltpu.SemaphoreType.REGULAR,
            pltpu.SemaphoreType.REGULAR,
            dma,
            dma,
            dma((chips - 1, pieces - 1)),
            dma((chips - 1, pieces - 1)),
            dma((chips - 1, 2)),
            dma((chips - 1, 2)),
            dma((chips - 1, pieces - 1)),
            dma((chips - 1, pieces - 1)),
            dma,
            dma,
            dma((n_sp,)),
            dma((n_sp, 2)),
            dma((chips, 2)),
            dma((chips,)),
        ],
        compiler_params=pltpu.CompilerParams(
            collective_id=0, has_side_effects=True, vmem_limit_bytes=VMEM_BYTES - room
        ),
    )(
        x, key_weight, value_weight, new_queries, lambdas.reshape(1, heads),
        head_gain.reshape(1, wide), out_weight, jnp.asarray(fine), jnp.asarray(coarse),
    )
    k, v, mixed = pl.pallas_call(
        deliver,
        out_shape=(
            jax.ShapeDtypeStruct(cache, bf16),
            jax.ShapeDtypeStruct(cache, bf16),
            jax.ShapeDtypeStruct((1, out_cols), bf16),
        ),
        in_specs=[vmem_spec] * 3,
        out_specs=(hbm_spec,) * 3,
        scratch_shapes=[dma((3,))],
        compiler_params=pltpu.CompilerParams(vmem_limit_bytes=2**20),
    )(k, v, mixed)
    full = (1, n_tp * rows, columns)
    return k.reshape(full), v.reshape(full), mixed


def solution(mesh):
    n_sp, n_tp = mesh.shape["sp"], mesh.shape["tp"]
    in_specs = (
        P("gr", ("sp", "tp"), None),
        P(None, "tp"),
        P(None, "tp"),
        P("gr", "tp"),
        P("tp"),
        P(),
        P("tp", None),
    )
    out_specs = (P("gr", "sp", "tp"), P("gr", "sp", "tp"), P("gr", "tp"))
    return jax.shard_map(
        functools.partial(on_device, n_sp, n_tp),
        mesh=mesh, in_specs=in_specs, out_specs=out_specs, check_vma=False,
    )
```

```python
import functools

import jax
import jax.numpy as jnp
import numpy as np
from jax import lax
from jax.experimental import pallas as pl
from jax.experimental.pallas import tpu as pltpu
from jax.sharding import PartitionSpec as P

MESH = pl.DeviceIdType.MESH
MAP_ROWS = 16
LANES = 128
VMEM_BYTES = 67043328
SMALL_BYTES = 16384
SLICES = (5, 2, 1)
RELAY_ROWS = 8


def kernel(
    n_sp, n_tp, heads, head_dim, chunk,
    x_ref, wk_ref, wv_ref, q_ref, lam_ref, gain_ref, wo_ref, fine_ref, coarse_ref,
    keys, values, mix_ref,
    xg, wk, wv, wo, q, lam, gain, fine, coarse, stats, part, parts, sums, turned_q, pick,
    relay_in, relay_out,
    load_sem, own_sem, up_sem, down_sem, near_send, near_recv, far_send, far_recv, twin_send, twin_recv,
    fwd_send, fwd_recv,
    in_send, in_recv, out_send, out_recv, back_send, back_recv,
    wo_send, wo_recv, st_send, st_recv, pt_send, pt_recv,
):
    sp = lax.axis_index("sp")
    tp = lax.axis_index("tp")
    rows, depth = x_ref.shape[1:]
    columns = wk.shape[1]
    wide = 2 * head_dim
    maps = 2 * heads
    steps = rows // chunk
    chips = n_tp // 2
    core = lax.rem(tp, 2)
    partner = tp + 1 - 2 * core
    is_lead = core == 1
    out_cols = mix_ref.shape[1]
    local_coarse = n_tp * steps
    last = steps - 1
    unit = depth // sum(SLICES)
    edges = [unit * sum(SLICES[:i]) for i in range(len(SLICES) + 1)]
    cuts = [slice(edges[i], edges[i + 1]) for i in range(len(SLICES))]
    pieces = [(j, slice(0, depth)) for j in range(last)] + [(last, cut) for cut in cuts]

    def piece_of(block, piece):
        j, cut = pieces[piece]
        return xg.at[block, pl.ds(j * chunk, chunk), pl.ds(cut.start, cut.stop - cut.start)]

    own_loads = [
        pltpu.make_async_copy(
            x_ref.at[0, pl.ds(j * chunk, chunk)], xg.at[tp, pl.ds(j * chunk, chunk)], own_sem.at[j]
        )
        for j in range(steps)
    ]
    loads = [
        pltpu.make_async_copy(q_ref, q, load_sem.at[5]),
        pltpu.make_async_copy(wk_ref, wk, load_sem.at[1]),
        pltpu.make_async_copy(wv_ref, wv, load_sem.at[2]),
        pltpu.make_async_copy(fine_ref, fine, load_sem.at[3]),
        pltpu.make_async_copy(
            coarse_ref.at[pl.ds(sp * local_coarse, local_coarse)], coarse, load_sem.at[4]
        ),
        pltpu.make_async_copy(lam_ref, lam, load_sem.at[6]),
        pltpu.make_async_copy(gain_ref, gain, load_sem.at[7]),
    ]
    own_wo = pltpu.make_async_copy(wo_ref, wo.at[pl.ds(columns, columns)], load_sem.at[8])
    lent_wo = pltpu.make_async_remote_copy(
        src_ref=wo_ref,
        dst_ref=wo.at[pl.ds(0, columns)],
        send_sem=wo_send,
        recv_sem=wo_recv,
        device_id={"tp": partner},
        device_id_type=MESH,
    )

    own_loads[0].start()
    barrier = pltpu.get_barrier_semaphore()
    for d in range(1, n_tp):
        pl.semaphore_signal(
            barrier, inc=1, device_id={"tp": lax.rem(tp + d, n_tp)}, device_id_type=MESH
        )
    has_lower = sp > 0
    has_upper = sp < n_sp - 1

    @pl.when(has_lower)
    def _():
        pl.semaphore_signal(barrier, inc=1, device_id={"sp": sp - 1}, device_id_type=MESH)

    @pl.when(has_upper)
    def _():
        pl.semaphore_signal(barrier, inc=1, device_id={"sp": sp + 1}, device_id_type=MESH)

    @pl.when(sp == 0)
    def _():
        pl.semaphore_signal(barrier, inc=1, device_id={"sp": n_sp - 1}, device_id_type=MESH)

    for load in own_loads[1:]:
        load.start()
    pl.semaphore_wait(
        barrier,
        n_tp - 1 + jnp.where(has_lower, 1, 0) + jnp.where(has_upper, 1, 0)
        + jnp.where(sp == n_sp - 1, 1, 0),
    )

    is_first, is_last = sp == 0, sp == n_sp - 1
    relayed = last - 1
    kept = chunk - RELAY_ROWS
    relay_rows = pl.ds(relayed * chunk + kept, RELAY_ROWS)

    def far_copy(d, p, count=chunk):
        j, cut = pieces[p]
        where = xg.at[tp, pl.ds(j * chunk, count), pl.ds(cut.start, cut.stop - cut.start)]
        return pltpu.make_async_remote_copy(
            src_ref=where,
            dst_ref=where,
            send_sem=far_send.at[d - 1, p],
            recv_sem=far_recv.at[d - 1, p],
            device_id={"tp": lax.rem(partner + 2 * d, n_tp)},
            device_id_type=MESH,
        )

    def far_do(d, p, act):
        if p == relayed:
            pl.when(is_last)(lambda: act(far_copy(d, p, kept)))
            pl.when(sp < n_sp - 1)(lambda: act(far_copy(d, p)))
        else:
            act(far_copy(d, p))

    def start_far(p):
        for d in range(1, chips):
            far_do(d, p, lambda copy: copy.start())

    to_first = pltpu.make_async_remote_copy(
        src_ref=xg.at[tp, relay_rows],
        dst_ref=relay_in,
        send_sem=in_send,
        recv_sem=in_recv,
        device_id={"sp": 0},
        device_id_type=MESH,
    )
    @pl.when(is_last)
    def _():
        own_loads[relayed].wait()
        to_first.start()

    for j in range(steps):
        if j == relayed:
            pl.when(sp < n_sp - 1)(own_loads[j].wait)
        else:
            own_loads[j].wait()
        if j < relayed:
            start_far(j)
    near = pltpu.make_async_remote_copy(
        src_ref=xg.at[tp],
        dst_ref=xg.at[tp],
        send_sem=near_send,
        recv_sem=near_recv,
        device_id={"tp": partner},
        device_id_type=MESH,
    )
    near.start()
    for load in loads:
        load.start()
    pl.when(is_lead)(own_wo.start)

    pl.when(has_lower)(lambda: pl.semaphore_wait(up_sem, 1))

    @pl.when(has_upper)
    def _():
        pl.semaphore_signal(up_sem, inc=1, device_id={"sp": sp + 1}, device_id_type=MESH)

    lane = lax.broadcasted_iota(jnp.int32, (chunk, wide), 1)
    low_half = lax.rem(lane, head_dim) < head_dim // 2

    def angles(block, j):
        base = coarse[block * steps + j]
        base_cos, base_sin = base[0:1, :], base[1:2, :]
        cosine = base_cos * fine[0] - base_sin * fine[1]
        sine = base_sin * fine[0] + base_cos * fine[1]
        return cosine, sine

    def swapped(raw):
        ahead = pltpu.roll(raw, wide - head_dim // 2, 1)
        behind = pltpu.roll(raw, head_dim // 2, 1)
        return jnp.where(low_half, ahead, behind)

    def settle(block, first, count, raw_keys, raw_values):
        values[block, first * chunk:(first + count) * chunk, :] = raw_values.astype(jnp.bfloat16)
        for i in range(count):
            cosine, sine = angles(block, first + i)
            for h in range(heads):
                raw = raw_keys[i * chunk:(i + 1) * chunk, h * wide:(h + 1) * wide]
                turned = raw * cosine + swapped(raw) * sine
                keys[
                    block, (first + i) * chunk:(first + i + 1) * chunk, h * wide:(h + 1) * wide
                ] = turned.astype(jnp.bfloat16)

    def product(block, first, count, cut):
        piece = xg[block, first * chunk:(first + count) * chunk, cut]
        raw_keys = jnp.dot(piece, wk[cut, :], preferred_element_type=jnp.float32)
        raw_values = jnp.dot(piece, wv[cut, :], preferred_element_type=jnp.float32)
        return raw_keys, raw_values

    def project(block, first, count):
        settle(block, first, count, *product(block, first, count, slice(0, depth)))

    for load in loads[:5]:
        load.wait()
    map_row = lax.broadcasted_iota(jnp.int32, (MAP_ROWS, columns), 0)
    map_col = lax.broadcasted_iota(jnp.int32, (MAP_ROWS, columns), 1) // head_dim
    spread = jnp.where(map_row == map_col, q[...].astype(jnp.float32), 0.0).astype(jnp.bfloat16)

    def weigh(highest, weight, rows_of_values):
        total = jnp.sum(weight, axis=1, keepdims=True)
        upper = weight.astype(jnp.bfloat16)
        lower = (weight - upper.astype(jnp.float32)).astype(jnp.bfloat16)
        read = jnp.dot(
            jnp.concatenate([upper, lower], axis=0), rows_of_values,
            preferred_element_type=jnp.float32,
        )
        return highest, total, read[:MAP_ROWS] + read[MAP_ROWS:]

    def merge(one, two):
        highest = jnp.maximum(one[0], two[0])
        fades = jnp.exp(one[0] - highest), jnp.exp(two[0] - highest)
        return (
            highest,
            one[1] * fades[0] + two[1] * fades[1],
            one[2] * fades[0] + two[2] * fades[1],
        )

    def attend(state, block, first, count):
        where = slice(first * chunk, (first + count) * chunk)
        score = lax.dot_general(
            spread, keys[block, where, :], (((1,), (1,)), ((), ())),
            preferred_element_type=jnp.float32,
        ) * head_dim ** (-0.5)
        highest = jnp.max(score, axis=1, keepdims=True)
        fresh = weigh(highest, jnp.exp(score - highest), values[block, where, :])
        return fresh if state is None else merge(state, fresh)

    def attend_raw(state, slots, raw_keys, raw_values):
        products = jnp.concatenate(
            [raw * turned_q[slot] for raw, slot in zip(raw_keys, slots)], axis=0
        )
        count = products.shape[0]
        upper = products.astype(jnp.bfloat16)
        lower = (products - upper.astype(jnp.float32)).astype(jnp.bfloat16)
        score = jnp.dot(
            jnp.concatenate([upper, lower], axis=0), pick[...], preferred_element_type=jnp.float32
        )
        score = score[:count] + score[count:]
        highest = jnp.max(score, axis=0, keepdims=True)
        room = -(-(count + 8) // LANES) * LANES - count
        across = jnp.transpose(
            jnp.concatenate(
                [jnp.exp(score - highest), jnp.broadcast_to(highest, (room, LANES))], axis=0
            )
        )[:MAP_ROWS]
        rows_of_values = jnp.concatenate(raw_values, axis=0).astype(jnp.bfloat16)
        fresh = weigh(across[:, count:count + 1], across[:, :count], rows_of_values)
        return merge(state, fresh)

    project(tp, 0, steps)
    state = attend(None, tp, 0, steps)

    near.wait_recv()
    project(partner, 0, steps)
    state = attend(state, partner, 0, steps)

    pl.when(has_upper)(lambda: pl.semaphore_wait(down_sem, 1))

    @pl.when(has_lower)
    def _():
        pl.semaphore_signal(down_sem, inc=1, device_id={"sp": sp - 1}, device_id_type=MESH)

    for load in loads[5:]:
        load.wait()
    map_of = lax.broadcasted_iota(jnp.int32, (maps, wide), 0)
    lam_row = jnp.zeros((maps, wide), jnp.float32)
    for h in range(heads):
        lam_row = jnp.where(map_of == 2 * h, lam[0:1, h:h + 1], lam_row)

    def relay_out_copy(d):
        return pltpu.make_async_remote_copy(
            src_ref=relay_in,
            dst_ref=relay_out.at[d - 1],
            send_sem=out_send.at[d - 1],
            recv_sem=out_recv.at[d - 1],
            device_id={"tp": lax.rem(partner + 2 * d, n_tp)},
            device_id_type=MESH,
        )

    def relay_back_copy(d):
        return pltpu.make_async_remote_copy(
            src_ref=relay_out.at[d - 1],
            dst_ref=xg.at[sources[d], relay_rows],
            send_sem=back_send.at[d - 1],
            recv_sem=back_recv.at[d - 1],
            device_id={"sp": n_sp - 1},
            device_id_type=MESH,
        )

    sources = {d: lax.rem(partner + n_tp - 2 * d, n_tp) for d in range(1, chips)}
    others = {d: sources[d] + 1 - 2 * lax.rem(sources[d], 2) for d in sources}
    forwards = {}

    pick_row = lax.broadcasted_iota(jnp.int32, (columns, LANES), 0) // head_dim
    pick_lane = lax.broadcasted_iota(jnp.int32, (columns, LANES), 1)
    pick[...] = jnp.where(pick_row == pick_lane, 1.0, 0.0).astype(jnp.bfloat16)
    for d in sources:
        for side, block in enumerate((sources[d], others[d])):
            cosine, sine = angles(block, last)
            for h in range(heads):
                query = jnp.broadcast_to(
                    q[0:1, h * wide:(h + 1) * wide].astype(jnp.float32), (chunk, wide)
                )
                turned_q[2 * (d - 1) + side, :, h * wide:(h + 1) * wide] = (
                    query * cosine - swapped(query) * sine
                ) * head_dim ** (-0.5)

    def forward(d, p):
        far_do(d, p, lambda copy: copy.wait_recv())
        if p == relayed:
            pl.when(is_last)(relay_back_copy(d).wait_recv)
        forwards[d, p] = pltpu.make_async_remote_copy(
            src_ref=piece_of(sources[d], p),
            dst_ref=piece_of(sources[d], p),
            send_sem=fwd_send.at[d - 1, p],
            recv_sem=fwd_recv.at[d - 1, p],
            device_id={"tp": partner},
            device_id_type=MESH,
        )
        forwards[d, p].start()

    twins = {}

    def send_rest():
        @pl.when(is_first)
        def _():
            to_first.wait_recv()
            for d in range(1, chips):
                relay_out_copy(d).start()

        for p in range(relayed, len(pieces) - 1):
            start_far(p)
        for d in range(1, chips):
            for target in range(2):
                twins[d, target] = pltpu.make_async_remote_copy(
                    src_ref=piece_of(tp, len(pieces) - 1),
                    dst_ref=piece_of(tp, len(pieces) - 1),
                    send_sem=twin_send.at[d - 1, target],
                    recv_sem=twin_recv.at[d - 1, core],
                    device_id={"tp": lax.rem(tp - core + 2 * d, n_tp) + target},
                    device_id_type=MESH,
                )
                twins[d, target].start()

    def hand_back():
        @pl.when(is_first)
        def _():
            for d in sources:
                relay_out_copy(d).wait_recv()
                relay_back_copy(d).start()

    for j in range(last):
        for d in sources:
            forward(d, j)
            project(sources[d], j, 1)
            state = attend(state, sources[d], j, 1)
            if d == chips - 1 and j == 0:
                send_rest()
            if d == chips - 1 and j == relayed - 1:
                hand_back()
                pl.when(core == 0)(lent_wo.start)
            forwards[d, j].wait_recv()
            project(others[d], j, 1)
            state = attend(state, others[d], j, 1)

    tail = slice(edges[1], depth)

    def add_first(slot, block):
        sums[slot, :, :columns], sums[slot, :, columns:] = product(block, last, 1, cuts[0])

    for d in sources:
        forward(d, last)
        add_first(2 * d - 2, sources[d])
    for i in range(1, len(cuts) - 1):
        for d in sources:
            forward(d, last + i)
    for d in sources:
        forwards[d, last].wait_recv()
        add_first(2 * d - 1, others[d])
    for d in sources:
        pair = (sources[d], others[d])
        for i in range(1, len(cuts) - 1):
            forwards[d, last + i].wait_recv()
        for source in range(2):
            pltpu.make_async_remote_copy(
                src_ref=piece_of(sources[d], len(pieces) - 1),
                dst_ref=piece_of(sources[d], len(pieces) - 1),
                send_sem=twin_send.at[d - 1, source],
                recv_sem=twin_recv.at[d - 1, source],
                device_id={"tp": partner},
                device_id_type=MESH,
            ).wait_recv()
        both = jnp.concatenate([xg[block, last * chunk:rows, tail] for block in pair], axis=0)
        raws = []
        for w, where in ((wk, slice(0, columns)), (wv, slice(columns, 2 * columns))):
            raw = jnp.dot(both, w[tail, :], preferred_element_type=jnp.float32)
            raws.append([
                raw[side * chunk:(side + 1) * chunk] + sums[2 * (d - 1) + side, :, where]
                for side in range(2)
            ])
        for side, block in enumerate(pair):
            settle(block, last, 1, raws[0][side], raws[1][side])
        state = attend_raw(state, (2 * d - 2, 2 * d - 1), *raws)

    highest, total, read = state
    head_of = lax.broadcasted_iota(jnp.int32, (MAP_ROWS, wide), 0) // 2
    own = jnp.zeros((MAP_ROWS, wide), jnp.float32)
    for h in range(heads):
        own = jnp.where(head_of == h, read[:, h * wide:(h + 1) * wide], own)
    lane_of = lax.broadcasted_iota(jnp.int32, (maps, wide), 1)
    stats[sp, core, 0] = own[:maps]
    stats[sp, core, 1] = jnp.where(
        lane_of == 0, highest[:maps], jnp.where(lane_of == 1, total[:maps], lam_row)
    )

    def stats_copy(target):
        d = lax.rem(target + n_sp - sp, n_sp)
        return pltpu.make_async_remote_copy(
            src_ref=stats.at[sp, core],
            dst_ref=stats.at[sp, core],
            send_sem=st_send.at[d],
            recv_sem=st_recv.at[d, core],
            device_id={"sp": target, "tp": tp + 1 - core},
            device_id_type=MESH,
        )

    def stats_arrival(d, source):
        return pltpu.make_async_remote_copy(
            src_ref=stats.at[sp, source],
            dst_ref=stats.at[sp, source],
            send_sem=st_send.at[d],
            recv_sem=st_recv.at[d, source],
            device_id={"tp": partner},
            device_id_type=MESH,
        )

    exchanges = []
    for k in range(n_sp - 1):
        up, down = k + jnp.where(k >= sp, 1, 0), n_sp - 1 - k - jnp.where(n_sp - 1 - k <= sp, 1, 0)
        exchanges.append(stats_copy(jnp.where(2 * sp >= n_sp, up, down)))
        exchanges[-1].start()
    pl.when(core == 0)(stats_copy(sp).start)

    def share_copy(d, target):
        chip = lax.rem(tp // 2 + d, chips)
        return pltpu.make_async_remote_copy(
            src_ref=part.at[d, target, pl.ds(0, 1)],
            dst_ref=parts.at[d, pl.ds(0, 1)],
            send_sem=pt_send.at[d, target],
            recv_sem=pt_recv.at[d],
            device_id={"tp": 2 * chip + target},
            device_id_type=MESH,
        )

    @pl.when(is_lead)
    def _():
        own_wo.wait()
        lent_wo.wait_recv()
        stats_arrival(0, 0).wait_recv()
        for d in range(1, n_sp):
            for source in range(2):
                stats_arrival(d, source).wait_recv()
        headed, scales = [], []
        row_of = lax.broadcasted_iota(jnp.int32, (2 * MAP_ROWS, wide), 0)
        for c in range(2):
            heights = stats[:, c, 1]
            tops = heights[:, :, 0:1]
            totals = heights[:, :, 1:2]
            factor = jnp.exp(tops - jnp.max(tops, axis=0, keepdims=True))
            reads = jnp.sum(stats[:, c, 0] * factor, axis=0) / jnp.sum(totals * factor, axis=0)
            diff = reads - heights[0, :, 2:3] * pltpu.roll(reads, maps - 1, 0)
            scales.append(lax.rsqrt(jnp.mean(diff * diff, axis=1, keepdims=True) + 1e-06))
            gained = diff * gain[...]
            headed += [
                jnp.where(
                    row_of == c * MAP_ROWS + h, gained[2 * h:2 * h + 1], 0.0
                ).astype(jnp.bfloat16)
                for h in range(heads)
            ]
        headed = jnp.concatenate(headed, axis=1)
        for d in list(range(1, chips)) + [0]:
            for target in range(2):
                column = (2 * lax.rem(tp // 2 + d, chips) + target) * out_cols
                first = pl.multiple_of(column, out_cols)
                shares = jnp.dot(
                    headed, wo[:, pl.ds(first, out_cols)], preferred_element_type=jnp.float32
                )
                both = 0.0
                for c in range(2):
                    group = 0.0
                    for h in range(heads):
                        row = c * MAP_ROWS + h
                        group = group + shares[row:row + 1] * scales[c][2 * h:2 * h + 1]
                    both = both + group.astype(jnp.bfloat16).astype(jnp.float32)
                part[d, target, 0:1] = both
                if d > 0 or target == 0:
                    share_copy(d, target).start()
        mixed = part[0, 1, 0:1]
        for d in range(1, chips):
            share_copy(d, 1).wait_recv()
            mixed = mixed + parts[d, 0:1]
        mix_ref[...] = mixed.astype(jnp.bfloat16)
        for d in range(chips):
            for target in range(2):
                if d > 0 or target == 0:
                    share_copy(d, target).wait_send()

    @pl.when(core == 0)
    def _():
        mixed = None
        for d in range(chips):
            share_copy(d, 1).wait_recv()
            mixed = parts[d, 0:1] if mixed is None else mixed + parts[d, 0:1]
        mix_ref[...] = mixed.astype(jnp.bfloat16)
        lent_wo.wait_send()
        stats_copy(sp).wait_send()

    near.wait_send()
    pl.when(is_last)(to_first.wait_send)

    @pl.when(is_first)
    def _():
        for d in sources:
            relay_out_copy(d).wait_send()
            relay_back_copy(d).wait_send()

    for d in sources:
        for p in range(len(pieces) - 1):
            far_do(d, p, lambda copy: copy.wait_send())
    for copy in [*twins.values(), *forwards.values(), *exchanges]:
        copy.wait_send()


def deliver(keys, values, mixed, key_out, value_out, mix_out, sem):
    copies = [
        pltpu.make_async_copy(source, target, sem.at[i])
        for i, (source, target) in enumerate(
            ((keys, key_out), (values, value_out), (mixed, mix_out))
        )
    ]
    for copy in copies:
        copy.start()
    for copy in copies:
        copy.wait()


def tables(length, chunk, head_dim):
    inverse = 1.0 / 10000.0 ** (np.arange(0, head_dim, 2) / head_dim)
    inverse = np.tile(inverse, 4)
    sign = np.tile(np.repeat([-1.0, 1.0], head_dim // 2), 2)

    def pair(positions, axis):
        angles = positions[:, None] * inverse[None, :]
        both = np.stack([np.cos(angles), np.sin(angles) * sign], axis=axis)
        return both.astype(np.float32)

    return pair(np.arange(chunk), 0), pair(np.arange(0, length, chunk), 1)


def on_device(n_sp, n_tp, x, key_weight, value_weight, new_queries, lambdas, head_gain, out_weight):
    heads = lambdas.shape[0]
    columns = key_weight.shape[1]
    head_dim = columns // (2 * heads)
    wide = 2 * head_dim
    seqs, rows, depth = x.shape
    assert seqs == 1
    chunk = rows // 4
    steps = rows // chunk
    chips = n_tp // 2
    pieces = steps - 1 + len(SLICES)
    out_cols = out_weight.shape[1] // n_tp
    fine, coarse = tables(n_sp * n_tp * rows, chunk, head_dim)
    hbm_spec = pl.BlockSpec(memory_space=pltpu.HBM)
    vmem_spec = pl.BlockSpec(memory_space=pltpu.VMEM)
    dma = pltpu.SemaphoreType.DMA
    bf16 = jnp.bfloat16
    f32 = jnp.float32
    room = 2 * n_tp * rows * columns * 2 + SMALL_BYTES
    cache = (n_tp, rows, columns)
    k, v, mixed = pl.pallas_call(
        functools.partial(kernel, n_sp, n_tp, heads, head_dim, chunk),
        out_shape=(
            pltpu.VMEM(cache, bf16),
            pltpu.VMEM(cache, bf16),
            pltpu.VMEM((1, out_cols), bf16),
        ),
        in_specs=[hbm_spec] * 9,
        out_specs=(vmem_spec,) * 3,
        scratch_shapes=[
            pltpu.VMEM((n_tp, rows, depth), bf16),
            pltpu.VMEM((depth, columns), bf16),
            pltpu.VMEM((depth, columns), bf16),
            pltpu.VMEM((2 * columns, out_weight.shape[1]), bf16),
            pltpu.VMEM((1, columns), bf16),
            pltpu.VMEM((1, heads), f32),
            pltpu.VMEM((1, wide), f32),
            pltpu.VMEM((2, chunk, wide), f32),
            pltpu.VMEM((n_tp * steps, 2, wide), f32),
            pltpu.VMEM((n_sp, 2, 2, 2 * heads, wide), f32),
            pltpu.VMEM((chips, 2, 8, out_cols), f32),
            pltpu.VMEM((chips, 8, out_cols), f32),
            pltpu.VMEM((2 * (chips - 1), chunk, 2 * columns), f32),
            pltpu.VMEM((2 * (chips - 1), chunk, columns), f32),
            pltpu.VMEM((columns, LANES), bf16),
            pltpu.VMEM((RELAY_ROWS, depth), bf16),
            pltpu.VMEM((chips - 1, RELAY_ROWS, depth), bf16),
            dma((9,)),
            dma((steps,)),
            pltpu.SemaphoreType.REGULAR,
            pltpu.SemaphoreType.REGULAR,
            dma,
            dma,
            dma((chips - 1, pieces - 1)),
            dma((chips - 1, pieces - 1)),
            dma((chips - 1, 2)),
            dma((chips - 1, 2)),
            dma((chips - 1, pieces - 1)),
            dma((chips - 1, pieces - 1)),
            dma,
            dma,
            dma((chips - 1,)),
            dma((chips - 1,)),
            dma((chips - 1,)),
            dma((chips - 1,)),
            dma,
            dma,
            dma((n_sp,)),
            dma((n_sp, 2)),
            dma((chips, 2)),
            dma((chips,)),
        ],
        compiler_params=pltpu.CompilerParams(
            collective_id=0, has_side_effects=True, vmem_limit_bytes=VMEM_BYTES - room
        ),
    )(
        x, key_weight, value_weight, new_queries, lambdas.reshape(1, heads),
        head_gain.reshape(1, wide), out_weight, jnp.asarray(fine), jnp.asarray(coarse),
    )
    k, v, mixed = pl.pallas_call(
        deliver,
        out_shape=(
            jax.ShapeDtypeStruct(cache, bf16),
            jax.ShapeDtypeStruct(cache, bf16),
            jax.ShapeDtypeStruct((1, out_cols), bf16),
        ),
        in_specs=[vmem_spec] * 3,
        out_specs=(hbm_spec,) * 3,
        scratch_shapes=[dma((3,))],
        compiler_params=pltpu.CompilerParams(vmem_limit_bytes=2**20),
    )(k, v, mixed)
    full = (1, n_tp * rows, columns)
    return k.reshape(full), v.reshape(full), mixed


def solution(mesh):
    n_sp, n_tp = mesh.shape["sp"], mesh.shape["tp"]
    in_specs = (
        P("gr", ("sp", "tp"), None),
        P(None, "tp"),
        P(None, "tp"),
        P("gr", "tp"),
        P("tp"),
        P(),
        P("tp", None),
    )
    out_specs = (P("gr", "sp", "tp"), P("gr", "sp", "tp"), P("gr", "tp"))
    return jax.shard_map(
        functools.partial(on_device, n_sp, n_tp),
        mesh=mesh, in_specs=in_specs, out_specs=out_specs, check_vma=False,
    )
```

```python
import functools

import jax
import jax.numpy as jnp
import numpy as np
from jax import lax
from jax.experimental import pallas as pl
from jax.experimental.pallas import tpu as pltpu
from jax.sharding import PartitionSpec as P

MESH = pl.DeviceIdType.MESH
MAP_ROWS = 16
LANES = 128
VMEM_BYTES = 67043328
SMALL_BYTES = 16384
SLICES = (5, 2, 1)
RELAY_ROWS = 8
HELPER = 1


def kernel(
    n_sp, n_tp, heads, head_dim, chunk,
    x_ref, wk_ref, wv_ref, q_ref, lam_ref, gain_ref, wo_ref, fine_ref, coarse_ref,
    keys, values, mix_ref,
    xg, wk, wv, wo, q, lam, gain, fine, coarse, stats, part, parts, sums, turned_q, pick,
    relay_in, relay_out,
    load_sem, own_sem, up_sem, down_sem, near_send, near_recv, far_send, far_recv, twin_send, twin_recv,
    fwd_send, fwd_recv,
    in_send, in_recv, out_send, out_recv, back_send, back_recv,
    wo_send, wo_recv, st_send, st_recv, pt_send, pt_recv,
):
    sp = lax.axis_index("sp")
    tp = lax.axis_index("tp")
    rows, depth = x_ref.shape[1:]
    columns = wk.shape[1]
    wide = 2 * head_dim
    maps = 2 * heads
    steps = rows // chunk
    chips = n_tp // 2
    core = lax.rem(tp, 2)
    partner = tp + 1 - 2 * core
    is_lead = core == 1
    out_cols = mix_ref.shape[1]
    local_coarse = n_tp * steps
    last = steps - 1
    unit = depth // sum(SLICES)
    edges = [unit * sum(SLICES[:i]) for i in range(len(SLICES) + 1)]
    cuts = [slice(edges[i], edges[i + 1]) for i in range(len(SLICES))]
    pieces = [(j, slice(0, depth)) for j in range(last)] + [(last, cut) for cut in cuts]

    def piece_of(block, piece):
        j, cut = pieces[piece]
        return xg.at[block, pl.ds(j * chunk, chunk), pl.ds(cut.start, cut.stop - cut.start)]

    own_loads = [
        pltpu.make_async_copy(
            x_ref.at[0, pl.ds(j * chunk, chunk)], xg.at[tp, pl.ds(j * chunk, chunk)], own_sem.at[j]
        )
        for j in range(steps)
    ]
    loads = [
        pltpu.make_async_copy(q_ref, q, load_sem.at[5]),
        pltpu.make_async_copy(wk_ref, wk, load_sem.at[1]),
        pltpu.make_async_copy(wv_ref, wv, load_sem.at[2]),
        pltpu.make_async_copy(fine_ref, fine, load_sem.at[3]),
        pltpu.make_async_copy(
            coarse_ref.at[pl.ds(sp * local_coarse, local_coarse)], coarse, load_sem.at[4]
        ),
        pltpu.make_async_copy(lam_ref, lam, load_sem.at[6]),
        pltpu.make_async_copy(gain_ref, gain, load_sem.at[7]),
    ]
    own_wo = pltpu.make_async_copy(wo_ref, wo.at[pl.ds(columns, columns)], load_sem.at[8])
    lent_wo = pltpu.make_async_remote_copy(
        src_ref=wo_ref,
        dst_ref=wo.at[pl.ds(0, columns)],
        send_sem=wo_send,
        recv_sem=wo_recv,
        device_id={"tp": partner},
        device_id_type=MESH,
    )

    own_loads[0].start()
    barrier = pltpu.get_barrier_semaphore()
    for d in range(1, n_tp):
        pl.semaphore_signal(
            barrier, inc=1, device_id={"tp": lax.rem(tp + d, n_tp)}, device_id_type=MESH
        )
    has_lower = sp > 0
    has_upper = sp < n_sp - 1

    @pl.when(has_lower)
    def _():
        pl.semaphore_signal(barrier, inc=1, device_id={"sp": sp - 1}, device_id_type=MESH)

    @pl.when(has_upper)
    def _():
        pl.semaphore_signal(barrier, inc=1, device_id={"sp": sp + 1}, device_id_type=MESH)

    @pl.when(sp == HELPER)
    def _():
        pl.semaphore_signal(barrier, inc=1, device_id={"sp": n_sp - 1}, device_id_type=MESH)

    for load in own_loads[1:]:
        load.start()
    pl.semaphore_wait(
        barrier,
        n_tp - 1 + jnp.where(has_lower, 1, 0) + jnp.where(has_upper, 1, 0)
        + jnp.where(sp == n_sp - 1, 1, 0),
    )

    is_helper, is_last = sp == HELPER, sp == n_sp - 1
    relayed = last - 1
    kept = chunk - RELAY_ROWS
    relay_rows = pl.ds(relayed * chunk + kept, RELAY_ROWS)

    def far_copy(d, p, count=chunk):
        j, cut = pieces[p]
        where = xg.at[tp, pl.ds(j * chunk, count), pl.ds(cut.start, cut.stop - cut.start)]
        return pltpu.make_async_remote_copy(
            src_ref=where,
            dst_ref=where,
            send_sem=far_send.at[d - 1, p],
            recv_sem=far_recv.at[d - 1, p],
            device_id={"tp": lax.rem(partner + 2 * d, n_tp)},
            device_id_type=MESH,
        )

    def far_do(d, p, act):
        if p == relayed:
            pl.when(is_last)(lambda: act(far_copy(d, p, kept)))
            pl.when(sp < n_sp - 1)(lambda: act(far_copy(d, p)))
        else:
            act(far_copy(d, p))

    def start_far(p):
        for d in range(1, chips):
            far_do(d, p, lambda copy: copy.start())

    to_helper = pltpu.make_async_remote_copy(
        src_ref=xg.at[tp, relay_rows],
        dst_ref=relay_in,
        send_sem=in_send,
        recv_sem=in_recv,
        device_id={"sp": HELPER},
        device_id_type=MESH,
    )
    @pl.when(is_last)
    def _():
        own_loads[relayed].wait()
        to_helper.start()

    for j in range(steps):
        if j == relayed:
            pl.when(sp < n_sp - 1)(own_loads[j].wait)
        else:
            own_loads[j].wait()
        if j < relayed:
            start_far(j)
    near = pltpu.make_async_remote_copy(
        src_ref=xg.at[tp],
        dst_ref=xg.at[tp],
        send_sem=near_send,
        recv_sem=near_recv,
        device_id={"tp": partner},
        device_id_type=MESH,
    )
    near.start()
    for load in loads:
        load.start()
    pl.when(is_lead)(own_wo.start)

    pl.when(has_lower)(lambda: pl.semaphore_wait(up_sem, 1))

    @pl.when(has_upper)
    def _():
        pl.semaphore_signal(up_sem, inc=1, device_id={"sp": sp + 1}, device_id_type=MESH)

    lane = lax.broadcasted_iota(jnp.int32, (chunk, wide), 1)
    low_half = lax.rem(lane, head_dim) < head_dim // 2

    def angles(block, j):
        base = coarse[block * steps + j]
        base_cos, base_sin = base[0:1, :], base[1:2, :]
        cosine = base_cos * fine[0] - base_sin * fine[1]
        sine = base_sin * fine[0] + base_cos * fine[1]
        return cosine, sine

    def swapped(raw):
        ahead = pltpu.roll(raw, wide - head_dim // 2, 1)
        behind = pltpu.roll(raw, head_dim // 2, 1)
        return jnp.where(low_half, ahead, behind)

    def settle(block, first, count, raw_keys, raw_values):
        values[block, first * chunk:(first + count) * chunk, :] = raw_values.astype(jnp.bfloat16)
        for i in range(count):
            cosine, sine = angles(block, first + i)
            for h in range(heads):
                raw = raw_keys[i * chunk:(i + 1) * chunk, h * wide:(h + 1) * wide]
                turned = raw * cosine + swapped(raw) * sine
                keys[
                    block, (first + i) * chunk:(first + i + 1) * chunk, h * wide:(h + 1) * wide
                ] = turned.astype(jnp.bfloat16)

    def product(block, first, count, cut):
        piece = xg[block, first * chunk:(first + count) * chunk, cut]
        raw_keys = jnp.dot(piece, wk[cut, :], preferred_element_type=jnp.float32)
        raw_values = jnp.dot(piece, wv[cut, :], preferred_element_type=jnp.float32)
        return raw_keys, raw_values

    def project(block, first, count):
        settle(block, first, count, *product(block, first, count, slice(0, depth)))

    for load in loads[:5]:
        load.wait()
    map_row = lax.broadcasted_iota(jnp.int32, (MAP_ROWS, columns), 0)
    map_col = lax.broadcasted_iota(jnp.int32, (MAP_ROWS, columns), 1) // head_dim
    spread = jnp.where(map_row == map_col, q[...].astype(jnp.float32), 0.0).astype(jnp.bfloat16)

    def weigh(highest, weight, rows_of_values):
        total = jnp.sum(weight, axis=1, keepdims=True)
        upper = weight.astype(jnp.bfloat16)
        lower = (weight - upper.astype(jnp.float32)).astype(jnp.bfloat16)
        read = jnp.dot(
            jnp.concatenate([upper, lower], axis=0), rows_of_values,
            preferred_element_type=jnp.float32,
        )
        return highest, total, read[:MAP_ROWS] + read[MAP_ROWS:]

    def merge(one, two):
        highest = jnp.maximum(one[0], two[0])
        fades = jnp.exp(one[0] - highest), jnp.exp(two[0] - highest)
        return (
            highest,
            one[1] * fades[0] + two[1] * fades[1],
            one[2] * fades[0] + two[2] * fades[1],
        )

    def attend(state, block, first, count):
        where = slice(first * chunk, (first + count) * chunk)
        score = lax.dot_general(
            spread, keys[block, where, :], (((1,), (1,)), ((), ())),
            preferred_element_type=jnp.float32,
        ) * head_dim ** (-0.5)
        highest = jnp.max(score, axis=1, keepdims=True)
        fresh = weigh(highest, jnp.exp(score - highest), values[block, where, :])
        return fresh if state is None else merge(state, fresh)

    def attend_raw(state, slots, raw_keys, raw_values):
        products = jnp.concatenate(
            [raw * turned_q[slot] for raw, slot in zip(raw_keys, slots)], axis=0
        )
        count = products.shape[0]
        upper = products.astype(jnp.bfloat16)
        lower = (products - upper.astype(jnp.float32)).astype(jnp.bfloat16)
        score = jnp.dot(
            jnp.concatenate([upper, lower], axis=0), pick[...], preferred_element_type=jnp.float32
        )
        score = score[:count] + score[count:]
        highest = jnp.max(score, axis=0, keepdims=True)
        room = -(-(count + 8) // LANES) * LANES - count
        across = jnp.transpose(
            jnp.concatenate(
                [jnp.exp(score - highest), jnp.broadcast_to(highest, (room, LANES))], axis=0
            )
        )[:MAP_ROWS]
        rows_of_values = jnp.concatenate(raw_values, axis=0).astype(jnp.bfloat16)
        fresh = weigh(across[:, count:count + 1], across[:, :count], rows_of_values)
        return merge(state, fresh)

    project(tp, 0, steps)
    state = attend(None, tp, 0, steps)

    near.wait_recv()
    project(partner, 0, steps)
    state = attend(state, partner, 0, steps)

    pl.when(has_upper)(lambda: pl.semaphore_wait(down_sem, 1))

    @pl.when(has_lower)
    def _():
        pl.semaphore_signal(down_sem, inc=1, device_id={"sp": sp - 1}, device_id_type=MESH)

    for load in loads[5:]:
        load.wait()
    map_of = lax.broadcasted_iota(jnp.int32, (maps, wide), 0)
    lam_row = jnp.zeros((maps, wide), jnp.float32)
    for h in range(heads):
        lam_row = jnp.where(map_of == 2 * h, lam[0:1, h:h + 1], lam_row)

    def relay_out_copy(d):
        return pltpu.make_async_remote_copy(
            src_ref=relay_in,
            dst_ref=relay_out.at[d - 1],
            send_sem=out_send.at[d - 1],
            recv_sem=out_recv.at[d - 1],
            device_id={"tp": lax.rem(partner + 2 * d, n_tp)},
            device_id_type=MESH,
        )

    def relay_back_copy(d):
        return pltpu.make_async_remote_copy(
            src_ref=relay_out.at[d - 1],
            dst_ref=xg.at[sources[d], relay_rows],
            send_sem=back_send.at[d - 1],
            recv_sem=back_recv.at[d - 1],
            device_id={"sp": n_sp - 1},
            device_id_type=MESH,
        )

    sources = {d: lax.rem(partner + n_tp - 2 * d, n_tp) for d in range(1, chips)}
    others = {d: sources[d] + 1 - 2 * lax.rem(sources[d], 2) for d in sources}
    forwards = {}

    pick_row = lax.broadcasted_iota(jnp.int32, (columns, LANES), 0) // head_dim
    pick_lane = lax.broadcasted_iota(jnp.int32, (columns, LANES), 1)
    pick[...] = jnp.where(pick_row == pick_lane, 1.0, 0.0).astype(jnp.bfloat16)
    for d in sources:
        for side, block in enumerate((sources[d], others[d])):
            cosine, sine = angles(block, last)
            for h in range(heads):
                query = jnp.broadcast_to(
                    q[0:1, h * wide:(h + 1) * wide].astype(jnp.float32), (chunk, wide)
                )
                turned_q[2 * (d - 1) + side, :, h * wide:(h + 1) * wide] = (
                    query * cosine - swapped(query) * sine
                ) * head_dim ** (-0.5)

    def forward(d, p):
        far_do(d, p, lambda copy: copy.wait_recv())
        if p == relayed:
            pl.when(is_last)(relay_back_copy(d).wait_recv)
        forwards[d, p] = pltpu.make_async_remote_copy(
            src_ref=piece_of(sources[d], p),
            dst_ref=piece_of(sources[d], p),
            send_sem=fwd_send.at[d - 1, p],
            recv_sem=fwd_recv.at[d - 1, p],
            device_id={"tp": partner},
            device_id_type=MESH,
        )
        forwards[d, p].start()

    twins = {}

    def send_rest():
        @pl.when(is_helper)
        def _():
            to_helper.wait_recv()
            for d in range(1, chips):
                relay_out_copy(d).start()

        for p in range(relayed, len(pieces) - 1):
            start_far(p)
        for d in range(1, chips):
            for target in range(2):
                twins[d, target] = pltpu.make_async_remote_copy(
                    src_ref=piece_of(tp, len(pieces) - 1),
                    dst_ref=piece_of(tp, len(pieces) - 1),
                    send_sem=twin_send.at[d - 1, target],
                    recv_sem=twin_recv.at[d - 1, core],
                    device_id={"tp": lax.rem(tp - core + 2 * d, n_tp) + target},
                    device_id_type=MESH,
                )
                twins[d, target].start()

    def hand_back():
        @pl.when(is_helper)
        def _():
            for d in sources:
                relay_out_copy(d).wait_recv()
                relay_back_copy(d).start()

    for j in range(last):
        for d in sources:
            forward(d, j)
            project(sources[d], j, 1)
            state = attend(state, sources[d], j, 1)
            if d == chips - 1 and j == 0:
                send_rest()
            if d == chips - 1 and j == relayed - 1:
                hand_back()
                pl.when(core == 0)(lent_wo.start)
            forwards[d, j].wait_recv()
            project(others[d], j, 1)
            state = attend(state, others[d], j, 1)

    tail = slice(edges[1], depth)

    def add_first(slot, block):
        sums[slot, :, :columns], sums[slot, :, columns:] = product(block, last, 1, cuts[0])

    for d in sources:
        forward(d, last)
        add_first(2 * d - 2, sources[d])
    for i in range(1, len(cuts) - 1):
        for d in sources:
            forward(d, last + i)
    for d in sources:
        forwards[d, last].wait_recv()
        add_first(2 * d - 1, others[d])
    for d in sources:
        pair = (sources[d], others[d])
        for i in range(1, len(cuts) - 1):
            forwards[d, last + i].wait_recv()
        for source in range(2):
            pltpu.make_async_remote_copy(
                src_ref=piece_of(sources[d], len(pieces) - 1),
                dst_ref=piece_of(sources[d], len(pieces) - 1),
                send_sem=twin_send.at[d - 1, source],
                recv_sem=twin_recv.at[d - 1, source],
                device_id={"tp": partner},
                device_id_type=MESH,
            ).wait_recv()
        both = jnp.concatenate([xg[block, last * chunk:rows, tail] for block in pair], axis=0)
        raws = []
        for w, where in ((wk, slice(0, columns)), (wv, slice(columns, 2 * columns))):
            raw = jnp.dot(both, w[tail, :], preferred_element_type=jnp.float32)
            raws.append([
                raw[side * chunk:(side + 1) * chunk] + sums[2 * (d - 1) + side, :, where]
                for side in range(2)
            ])
        for side, block in enumerate(pair):
            settle(block, last, 1, raws[0][side], raws[1][side])
        state = attend_raw(state, (2 * d - 2, 2 * d - 1), *raws)

    highest, total, read = state
    head_of = lax.broadcasted_iota(jnp.int32, (MAP_ROWS, wide), 0) // 2
    own = jnp.zeros((MAP_ROWS, wide), jnp.float32)
    for h in range(heads):
        own = jnp.where(head_of == h, read[:, h * wide:(h + 1) * wide], own)
    lane_of = lax.broadcasted_iota(jnp.int32, (maps, wide), 1)
    stats[sp, core, 0] = own[:maps]
    stats[sp, core, 1] = jnp.where(
        lane_of == 0, highest[:maps], jnp.where(lane_of == 1, total[:maps], lam_row)
    )

    def stats_copy(target):
        d = lax.rem(target + n_sp - sp, n_sp)
        return pltpu.make_async_remote_copy(
            src_ref=stats.at[sp, core],
            dst_ref=stats.at[sp, core],
            send_sem=st_send.at[d],
            recv_sem=st_recv.at[d, core],
            device_id={"sp": target, "tp": tp + 1 - core},
            device_id_type=MESH,
        )

    def stats_arrival(d, source):
        return pltpu.make_async_remote_copy(
            src_ref=stats.at[sp, source],
            dst_ref=stats.at[sp, source],
            send_sem=st_send.at[d],
            recv_sem=st_recv.at[d, source],
            device_id={"tp": partner},
            device_id_type=MESH,
        )

    exchanges = []
    for k in range(n_sp - 1):
        up, down = k + jnp.where(k >= sp, 1, 0), n_sp - 1 - k - jnp.where(n_sp - 1 - k <= sp, 1, 0)
        exchanges.append(stats_copy(jnp.where(2 * sp >= n_sp, up, down)))
        exchanges[-1].start()
    pl.when(core == 0)(stats_copy(sp).start)

    def share_copy(d, target):
        chip = lax.rem(tp // 2 + d, chips)
        return pltpu.make_async_remote_copy(
            src_ref=part.at[d, target, pl.ds(0, 1)],
            dst_ref=parts.at[d, pl.ds(0, 1)],
            send_sem=pt_send.at[d, target],
            recv_sem=pt_recv.at[d],
            device_id={"tp": 2 * chip + target},
            device_id_type=MESH,
        )

    near.wait_send()
    pl.when(is_last)(to_helper.wait_send)

    @pl.when(is_helper)
    def _():
        for d in sources:
            relay_out_copy(d).wait_send()
            relay_back_copy(d).wait_send()

    for d in sources:
        for p in range(len(pieces) - 1):
            far_do(d, p, lambda copy: copy.wait_send())
    for copy in [*twins.values(), *forwards.values(), *exchanges]:
        copy.wait_send()

    @pl.when(is_lead)
    def _():
        own_wo.wait()
        lent_wo.wait_recv()
        stats_arrival(0, 0).wait_recv()
        for d in range(1, n_sp):
            for source in range(2):
                stats_arrival(d, source).wait_recv()
        headed, scales = [], []
        row_of = lax.broadcasted_iota(jnp.int32, (2 * MAP_ROWS, wide), 0)
        for c in range(2):
            heights = stats[:, c, 1]
            tops = heights[:, :, 0:1]
            totals = heights[:, :, 1:2]
            factor = jnp.exp(tops - jnp.max(tops, axis=0, keepdims=True))
            reads = jnp.sum(stats[:, c, 0] * factor, axis=0) / jnp.sum(totals * factor, axis=0)
            diff = reads - heights[0, :, 2:3] * pltpu.roll(reads, maps - 1, 0)
            scales.append(lax.rsqrt(jnp.mean(diff * diff, axis=1, keepdims=True) + 1e-06))
            gained = diff * gain[...]
            headed += [
                jnp.where(
                    row_of == c * MAP_ROWS + h, gained[2 * h:2 * h + 1], 0.0
                ).astype(jnp.bfloat16)
                for h in range(heads)
            ]
        headed = jnp.concatenate(headed, axis=1)
        for d in list(range(1, chips)) + [0]:
            for target in range(2):
                column = (2 * lax.rem(tp // 2 + d, chips) + target) * out_cols
                first = pl.multiple_of(column, out_cols)
                shares = jnp.dot(
                    headed, wo[:, pl.ds(first, out_cols)], preferred_element_type=jnp.float32
                )
                both = 0.0
                for c in range(2):
                    group = 0.0
                    for h in range(heads):
                        row = c * MAP_ROWS + h
                        group = group + shares[row:row + 1] * scales[c][2 * h:2 * h + 1]
                    both = both + group.astype(jnp.bfloat16).astype(jnp.float32)
                part[d, target, 0:1] = both
                if d > 0 or target == 0:
                    share_copy(d, target).start()
        mixed = part[0, 1, 0:1]
        for d in range(1, chips):
            share_copy(d, 1).wait_recv()
            mixed = mixed + parts[d, 0:1]
        mix_ref[...] = mixed.astype(jnp.bfloat16)
        for d in range(chips):
            for target in range(2):
                if d > 0 or target == 0:
                    share_copy(d, target).wait_send()

    @pl.when(core == 0)
    def _():
        lent_wo.wait_send()
        stats_copy(sp).wait_send()
        mixed = None
        for d in range(chips):
            share_copy(d, 1).wait_recv()
            mixed = parts[d, 0:1] if mixed is None else mixed + parts[d, 0:1]
        mix_ref[...] = mixed.astype(jnp.bfloat16)


def deliver(keys, values, mixed, key_out, value_out, mix_out, sem):
    copies = [
        pltpu.make_async_copy(source, target, sem.at[i])
        for i, (source, target) in enumerate(
            ((keys, key_out), (values, value_out), (mixed, mix_out))
        )
    ]
    for copy in copies:
        copy.start()
    for copy in copies:
        copy.wait()


def tables(length, chunk, head_dim):
    inverse = 1.0 / 10000.0 ** (np.arange(0, head_dim, 2) / head_dim)
    inverse = np.tile(inverse, 4)
    sign = np.tile(np.repeat([-1.0, 1.0], head_dim // 2), 2)

    def pair(positions, axis):
        angles = positions[:, None] * inverse[None, :]
        both = np.stack([np.cos(angles), np.sin(angles) * sign], axis=axis)
        return both.astype(np.float32)

    return pair(np.arange(chunk), 0), pair(np.arange(0, length, chunk), 1)


def on_device(n_sp, n_tp, x, key_weight, value_weight, new_queries, lambdas, head_gain, out_weight):
    heads = lambdas.shape[0]
    columns = key_weight.shape[1]
    head_dim = columns // (2 * heads)
    wide = 2 * head_dim
    seqs, rows, depth = x.shape
    assert seqs == 1 and n_sp > HELPER + 1
    chunk = rows // 4
    steps = rows // chunk
    chips = n_tp // 2
    pieces = steps - 1 + len(SLICES)
    out_cols = out_weight.shape[1] // n_tp
    fine, coarse = tables(n_sp * n_tp * rows, chunk, head_dim)
    hbm_spec = pl.BlockSpec(memory_space=pltpu.HBM)
    vmem_spec = pl.BlockSpec(memory_space=pltpu.VMEM)
    dma = pltpu.SemaphoreType.DMA
    bf16 = jnp.bfloat16
    f32 = jnp.float32
    room = 2 * n_tp * rows * columns * 2 + SMALL_BYTES
    cache = (n_tp, rows, columns)
    k, v, mixed = pl.pallas_call(
        functools.partial(kernel, n_sp, n_tp, heads, head_dim, chunk),
        out_shape=(
            pltpu.VMEM(cache, bf16),
            pltpu.VMEM(cache, bf16),
            pltpu.VMEM((1, out_cols), bf16),
        ),
        in_specs=[hbm_spec] * 9,
        out_specs=(vmem_spec,) * 3,
        scratch_shapes=[
            pltpu.VMEM((n_tp, rows, depth), bf16),
            pltpu.VMEM((depth, columns), bf16),
            pltpu.VMEM((depth, columns), bf16),
            pltpu.VMEM((2 * columns, out_weight.shape[1]), bf16),
            pltpu.VMEM((1, columns), bf16),
            pltpu.VMEM((1, heads), f32),
            pltpu.VMEM((1, wide), f32),
            pltpu.VMEM((2, chunk, wide), f32),
            pltpu.VMEM((n_tp * steps, 2, wide), f32),
            pltpu.VMEM((n_sp, 2, 2, 2 * heads, wide), f32),
            pltpu.VMEM((chips, 2, 8, out_cols), f32),
            pltpu.VMEM((chips, 8, out_cols), f32),
            pltpu.VMEM((2 * (chips - 1), chunk, 2 * columns), f32),
            pltpu.VMEM((2 * (chips - 1), chunk, columns), f32),
            pltpu.VMEM((columns, LANES), bf16),
            pltpu.VMEM((RELAY_ROWS, depth), bf16),
            pltpu.VMEM((chips - 1, RELAY_ROWS, depth), bf16),
            dma((9,)),
            dma((steps,)),
            pltpu.SemaphoreType.REGULAR,
            pltpu.SemaphoreType.REGULAR,
            dma,
            dma,
            dma((chips - 1, pieces - 1)),
            dma((chips - 1, pieces - 1)),
            dma((chips - 1, 2)),
            dma((chips - 1, 2)),
            dma((chips - 1, pieces - 1)),
            dma((chips - 1, pieces - 1)),
            dma,
            dma,
            dma((chips - 1,)),
            dma((chips - 1,)),
            dma((chips - 1,)),
            dma((chips - 1,)),
            dma,
            dma,
            dma((n_sp,)),
            dma((n_sp, 2)),
            dma((chips, 2)),
            dma((chips,)),
        ],
        compiler_params=pltpu.CompilerParams(
            collective_id=0, has_side_effects=True, vmem_limit_bytes=VMEM_BYTES - room
        ),
    )(
        x, key_weight, value_weight, new_queries, lambdas.reshape(1, heads),
        head_gain.reshape(1, wide), out_weight, jnp.asarray(fine), jnp.asarray(coarse),
    )
    k, v, mixed = pl.pallas_call(
        deliver,
        out_shape=(
            jax.ShapeDtypeStruct(cache, bf16),
            jax.ShapeDtypeStruct(cache, bf16),
            jax.ShapeDtypeStruct((1, out_cols), bf16),
        ),
        in_specs=[vmem_spec] * 3,
        out_specs=(hbm_spec,) * 3,
        scratch_shapes=[dma((3,))],
        compiler_params=pltpu.CompilerParams(vmem_limit_bytes=2**20),
    )(k, v, mixed)
    full = (1, n_tp * rows, columns)
    return k.reshape(full), v.reshape(full), mixed


def solution(mesh):
    n_sp, n_tp = mesh.shape["sp"], mesh.shape["tp"]
    in_specs = (
        P("gr", ("sp", "tp"), None),
        P(None, "tp"),
        P(None, "tp"),
        P("gr", "tp"),
        P("tp"),
        P(),
        P("tp", None),
    )
    out_specs = (P("gr", "sp", "tp"), P("gr", "sp", "tp"), P("gr", "tp"))
    return jax.shard_map(
        functools.partial(on_device, n_sp, n_tp),
        mesh=mesh, in_specs=in_specs, out_specs=out_specs, check_vma=False,
    )
```

```python
import functools

import jax
import jax.numpy as jnp
import numpy as np
from jax import lax
from jax.experimental import pallas as pl
from jax.experimental.pallas import tpu as pltpu
from jax.sharding import PartitionSpec as P

MESH = pl.DeviceIdType.MESH
MAP_ROWS = 16
LANES = 128
VMEM_BYTES = 67043328
SMALL_BYTES = 16384
SLICES = (5, 2, 1)
RELAY_ROWS = 8
HELPER = 1


def kernel(
    n_sp, n_tp, heads, head_dim, chunk,
    x_ref, wk_ref, wv_ref, q_ref, lam_ref, gain_ref, wo_ref, fine_ref, coarse_ref,
    keys, values, mix_ref,
    xg, wk, wv, wo, q, lam, gain, fine, coarse, stats, part, parts, sums, turned_q, pick,
    relay_in, relay_out,
    load_sem, own_sem, up_sem, down_sem, near_send, near_recv, far_send, far_recv, twin_send, twin_recv,
    fwd_send, fwd_recv,
    in_send, in_recv, out_send, out_recv, back_send, back_recv,
    wo_send, wo_recv, st_send, st_recv, pt_send, pt_recv,
):
    sp = lax.axis_index("sp")
    tp = lax.axis_index("tp")
    rows, depth = x_ref.shape[1:]
    columns = wk.shape[1]
    wide = 2 * head_dim
    maps = 2 * heads
    steps = rows // chunk
    chips = n_tp // 2
    core = lax.rem(tp, 2)
    partner = tp + 1 - 2 * core
    is_lead = core == 1
    out_cols = mix_ref.shape[1]
    local_coarse = n_tp * steps
    last = steps - 1
    unit = depth // sum(SLICES)
    edges = [unit * sum(SLICES[:i]) for i in range(len(SLICES) + 1)]
    cuts = [slice(edges[i], edges[i + 1]) for i in range(len(SLICES))]
    pieces = [(j, slice(0, depth)) for j in range(last)] + [(last, cut) for cut in cuts]

    def piece_of(block, piece):
        j, cut = pieces[piece]
        return xg.at[block, pl.ds(j * chunk, chunk), pl.ds(cut.start, cut.stop - cut.start)]

    own_loads = [
        pltpu.make_async_copy(
            x_ref.at[0, pl.ds(j * chunk, chunk)], xg.at[tp, pl.ds(j * chunk, chunk)], own_sem.at[j]
        )
        for j in range(steps)
    ]
    loads = [
        pltpu.make_async_copy(q_ref, q, load_sem.at[5]),
        pltpu.make_async_copy(wk_ref, wk, load_sem.at[1]),
        pltpu.make_async_copy(wv_ref, wv, load_sem.at[2]),
        pltpu.make_async_copy(fine_ref, fine, load_sem.at[3]),
        pltpu.make_async_copy(
            coarse_ref.at[pl.ds(sp * local_coarse, local_coarse)], coarse, load_sem.at[4]
        ),
        pltpu.make_async_copy(lam_ref, lam, load_sem.at[6]),
        pltpu.make_async_copy(gain_ref, gain, load_sem.at[7]),
    ]
    own_wo = pltpu.make_async_copy(wo_ref, wo.at[pl.ds(columns, columns)], load_sem.at[8])
    lent_wo = pltpu.make_async_remote_copy(
        src_ref=wo_ref,
        dst_ref=wo.at[pl.ds(0, columns)],
        send_sem=wo_send,
        recv_sem=wo_recv,
        device_id={"tp": partner},
        device_id_type=MESH,
    )

    own_loads[0].start()
    barrier = pltpu.get_barrier_semaphore()
    for d in range(1, n_tp):
        pl.semaphore_signal(
            barrier, inc=1, device_id={"tp": lax.rem(tp + d, n_tp)}, device_id_type=MESH
        )
    has_lower = sp > 0
    has_upper = sp < n_sp - 1

    @pl.when(has_lower)
    def _():
        pl.semaphore_signal(barrier, inc=1, device_id={"sp": sp - 1}, device_id_type=MESH)

    @pl.when(has_upper)
    def _():
        pl.semaphore_signal(barrier, inc=1, device_id={"sp": sp + 1}, device_id_type=MESH)

    @pl.when(sp == HELPER)
    def _():
        pl.semaphore_signal(barrier, inc=1, device_id={"sp": n_sp - 1}, device_id_type=MESH)

    for load in own_loads[1:]:
        load.start()
    pl.semaphore_wait(
        barrier,
        n_tp - 1 + jnp.where(has_lower, 1, 0) + jnp.where(has_upper, 1, 0)
        + jnp.where(sp == n_sp - 1, 1, 0),
    )

    is_helper, is_last = sp == HELPER, sp == n_sp - 1
    relayed = last - 1
    kept = chunk - RELAY_ROWS
    relay_rows = pl.ds(relayed * chunk + kept, RELAY_ROWS)

    def far_copy(d, p, count=chunk):
        j, cut = pieces[p]
        where = xg.at[tp, pl.ds(j * chunk, count), pl.ds(cut.start, cut.stop - cut.start)]
        return pltpu.make_async_remote_copy(
            src_ref=where,
            dst_ref=where,
            send_sem=far_send.at[d - 1, p],
            recv_sem=far_recv.at[d - 1, p],
            device_id={"tp": lax.rem(partner + 2 * d, n_tp)},
            device_id_type=MESH,
        )

    def far_do(d, p, act):
        if p == relayed:
            pl.when(is_last)(lambda: act(far_copy(d, p, kept)))
            pl.when(sp < n_sp - 1)(lambda: act(far_copy(d, p)))
        else:
            act(far_copy(d, p))

    def start_far(p):
        for d in range(1, chips):
            far_do(d, p, lambda copy: copy.start())

    to_helper = pltpu.make_async_remote_copy(
        src_ref=xg.at[tp, relay_rows],
        dst_ref=relay_in,
        send_sem=in_send,
        recv_sem=in_recv,
        device_id={"sp": HELPER},
        device_id_type=MESH,
    )
    @pl.when(is_last)
    def _():
        own_loads[relayed].wait()
        to_helper.start()

    for j in range(steps):
        if j == relayed:
            pl.when(sp < n_sp - 1)(own_loads[j].wait)
        else:
            own_loads[j].wait()
        if j < relayed:
            start_far(j)
    near = pltpu.make_async_remote_copy(
        src_ref=xg.at[tp],
        dst_ref=xg.at[tp],
        send_sem=near_send,
        recv_sem=near_recv,
        device_id={"tp": partner},
        device_id_type=MESH,
    )
    near.start()
    for load in loads:
        load.start()
    pl.when(is_lead)(own_wo.start)

    pl.when(has_lower)(lambda: pl.semaphore_wait(up_sem, 1))

    @pl.when(has_upper)
    def _():
        pl.semaphore_signal(up_sem, inc=1, device_id={"sp": sp + 1}, device_id_type=MESH)

    lane = lax.broadcasted_iota(jnp.int32, (chunk, wide), 1)
    low_half = lax.rem(lane, head_dim) < head_dim // 2

    def angles(block, j):
        base = coarse[block * steps + j]
        base_cos, base_sin = base[0:1, :], base[1:2, :]
        cosine = base_cos * fine[0] - base_sin * fine[1]
        sine = base_sin * fine[0] + base_cos * fine[1]
        return cosine, sine

    def swapped(raw):
        ahead = pltpu.roll(raw, wide - head_dim // 2, 1)
        behind = pltpu.roll(raw, head_dim // 2, 1)
        return jnp.where(low_half, ahead, behind)

    def settle(block, first, count, raw_keys, raw_values):
        values[block, first * chunk:(first + count) * chunk, :] = raw_values.astype(jnp.bfloat16)
        for i in range(count):
            cosine, sine = angles(block, first + i)
            for h in range(heads):
                raw = raw_keys[i * chunk:(i + 1) * chunk, h * wide:(h + 1) * wide]
                turned = raw * cosine + swapped(raw) * sine
                keys[
                    block, (first + i) * chunk:(first + i + 1) * chunk, h * wide:(h + 1) * wide
                ] = turned.astype(jnp.bfloat16)

    def product(block, first, count, cut):
        piece = xg[block, first * chunk:(first + count) * chunk, cut]
        raw_keys = jnp.dot(piece, wk[cut, :], preferred_element_type=jnp.float32)
        raw_values = jnp.dot(piece, wv[cut, :], preferred_element_type=jnp.float32)
        return raw_keys, raw_values

    def project(block, first, count):
        settle(block, first, count, *product(block, first, count, slice(0, depth)))

    for load in loads[:5]:
        load.wait()
    map_row = lax.broadcasted_iota(jnp.int32, (MAP_ROWS, columns), 0)
    map_col = lax.broadcasted_iota(jnp.int32, (MAP_ROWS, columns), 1) // head_dim
    spread = jnp.where(map_row == map_col, q[...].astype(jnp.float32), 0.0).astype(jnp.bfloat16)

    def weigh(highest, weight, rows_of_values):
        total = jnp.sum(weight, axis=1, keepdims=True)
        upper = weight.astype(jnp.bfloat16)
        lower = (weight - upper.astype(jnp.float32)).astype(jnp.bfloat16)
        read = jnp.dot(
            jnp.concatenate([upper, lower], axis=0), rows_of_values,
            preferred_element_type=jnp.float32,
        )
        return highest, total, read[:MAP_ROWS] + read[MAP_ROWS:]

    def merge(one, two):
        highest = jnp.maximum(one[0], two[0])
        fades = jnp.exp(one[0] - highest), jnp.exp(two[0] - highest)
        return (
            highest,
            one[1] * fades[0] + two[1] * fades[1],
            one[2] * fades[0] + two[2] * fades[1],
        )

    def attend(state, block, first, count):
        where = slice(first * chunk, (first + count) * chunk)
        score = lax.dot_general(
            spread, keys[block, where, :], (((1,), (1,)), ((), ())),
            preferred_element_type=jnp.float32,
        ) * head_dim ** (-0.5)
        highest = jnp.max(score, axis=1, keepdims=True)
        fresh = weigh(highest, jnp.exp(score - highest), values[block, where, :])
        return fresh if state is None else merge(state, fresh)

    def attend_raw(state, slots, raw_keys, raw_values):
        products = jnp.concatenate(
            [raw * turned_q[slot] for raw, slot in zip(raw_keys, slots)], axis=0
        )
        count = products.shape[0]
        upper = products.astype(jnp.bfloat16)
        lower = (products - upper.astype(jnp.float32)).astype(jnp.bfloat16)
        score = jnp.dot(
            jnp.concatenate([upper, lower], axis=0), pick[...], preferred_element_type=jnp.float32
        )
        score = score[:count] + score[count:]
        highest = jnp.max(score, axis=0, keepdims=True)
        room = -(-(count + 8) // LANES) * LANES - count
        across = jnp.transpose(
            jnp.concatenate(
                [jnp.exp(score - highest), jnp.broadcast_to(highest, (room, LANES))], axis=0
            )
        )[:MAP_ROWS]
        rows_of_values = jnp.concatenate(raw_values, axis=0).astype(jnp.bfloat16)
        fresh = weigh(across[:, count:count + 1], across[:, :count], rows_of_values)
        return merge(state, fresh)

    project(tp, 0, steps)
    state = attend(None, tp, 0, steps)

    near.wait_recv()
    project(partner, 0, steps)
    state = attend(state, partner, 0, steps)

    pl.when(has_upper)(lambda: pl.semaphore_wait(down_sem, 1))

    @pl.when(has_lower)
    def _():
        pl.semaphore_signal(down_sem, inc=1, device_id={"sp": sp - 1}, device_id_type=MESH)

    for load in loads[5:]:
        load.wait()
    map_of = lax.broadcasted_iota(jnp.int32, (maps, wide), 0)
    lam_row = jnp.zeros((maps, wide), jnp.float32)
    for h in range(heads):
        lam_row = jnp.where(map_of == 2 * h, lam[0:1, h:h + 1], lam_row)

    def relay_out_copy(d):
        return pltpu.make_async_remote_copy(
            src_ref=relay_in,
            dst_ref=relay_out.at[d - 1],
            send_sem=out_send.at[d - 1],
            recv_sem=out_recv.at[d - 1],
            device_id={"tp": lax.rem(partner + 2 * d, n_tp)},
            device_id_type=MESH,
        )

    def relay_back_copy(d):
        return pltpu.make_async_remote_copy(
            src_ref=relay_out.at[d - 1],
            dst_ref=xg.at[sources[d], relay_rows],
            send_sem=back_send.at[d - 1],
            recv_sem=back_recv.at[d - 1],
            device_id={"sp": n_sp - 1},
            device_id_type=MESH,
        )

    sources = {d: lax.rem(partner + n_tp - 2 * d, n_tp) for d in range(1, chips)}
    others = {d: sources[d] + 1 - 2 * lax.rem(sources[d], 2) for d in sources}
    forwards = {}

    pick_row = lax.broadcasted_iota(jnp.int32, (columns, LANES), 0) // head_dim
    pick_lane = lax.broadcasted_iota(jnp.int32, (columns, LANES), 1)
    pick[...] = jnp.where(pick_row == pick_lane, 1.0, 0.0).astype(jnp.bfloat16)
    for d in sources:
        for side, block in enumerate((sources[d], others[d])):
            cosine, sine = angles(block, last)
            for h in range(heads):
                query = jnp.broadcast_to(
                    q[0:1, h * wide:(h + 1) * wide].astype(jnp.float32), (chunk, wide)
                )
                turned_q[2 * (d - 1) + side, :, h * wide:(h + 1) * wide] = (
                    query * cosine - swapped(query) * sine
                ) * head_dim ** (-0.5)

    def forward(d, p):
        far_do(d, p, lambda copy: copy.wait_recv())
        if p == relayed:
            pl.when(is_last)(relay_back_copy(d).wait_recv)
        forwards[d, p] = pltpu.make_async_remote_copy(
            src_ref=piece_of(sources[d], p),
            dst_ref=piece_of(sources[d], p),
            send_sem=fwd_send.at[d - 1, p],
            recv_sem=fwd_recv.at[d - 1, p],
            device_id={"tp": partner},
            device_id_type=MESH,
        )
        forwards[d, p].start()

    twins = {}

    def send_rest():
        @pl.when(is_helper)
        def _():
            to_helper.wait_recv()
            for d in range(1, chips):
                relay_out_copy(d).start()

        for p in range(relayed, len(pieces) - 1):
            start_far(p)
        for d in range(1, chips):
            for target in range(2):
                twins[d, target] = pltpu.make_async_remote_copy(
                    src_ref=piece_of(tp, len(pieces) - 1),
                    dst_ref=piece_of(tp, len(pieces) - 1),
                    send_sem=twin_send.at[d - 1, target],
                    recv_sem=twin_recv.at[d - 1, core],
                    device_id={"tp": lax.rem(tp - core + 2 * d, n_tp) + target},
                    device_id_type=MESH,
                )
                twins[d, target].start()

    def hand_back():
        @pl.when(is_helper)
        def _():
            for d in sources:
                relay_out_copy(d).wait_recv()
                relay_back_copy(d).start()

    send_rest()
    for j in range(last):
        for d in sources:
            forward(d, j)
            project(sources[d], j, 1)
            state = attend(state, sources[d], j, 1)
            if d == chips - 1 and j == relayed - 1:
                hand_back()
                pl.when(core == 0)(lent_wo.start)
            forwards[d, j].wait_recv()
            project(others[d], j, 1)
            state = attend(state, others[d], j, 1)

    tail = slice(edges[1], depth)

    def add_first(slot, block):
        sums[slot, :, :columns], sums[slot, :, columns:] = product(block, last, 1, cuts[0])

    for d in sources:
        forward(d, last)
        add_first(2 * d - 2, sources[d])
    for i in range(1, len(cuts) - 1):
        for d in sources:
            forward(d, last + i)
    for d in sources:
        forwards[d, last].wait_recv()
        add_first(2 * d - 1, others[d])
    for d in sources:
        pair = (sources[d], others[d])
        for i in range(1, len(cuts) - 1):
            forwards[d, last + i].wait_recv()
        for source in range(2):
            pltpu.make_async_remote_copy(
                src_ref=piece_of(sources[d], len(pieces) - 1),
                dst_ref=piece_of(sources[d], len(pieces) - 1),
                send_sem=twin_send.at[d - 1, source],
                recv_sem=twin_recv.at[d - 1, source],
                device_id={"tp": partner},
                device_id_type=MESH,
            ).wait_recv()
        both = jnp.concatenate([xg[block, last * chunk:rows, tail] for block in pair], axis=0)
        raws = []
        for w, where in ((wk, slice(0, columns)), (wv, slice(columns, 2 * columns))):
            raw = jnp.dot(both, w[tail, :], preferred_element_type=jnp.float32)
            raws.append([
                raw[side * chunk:(side + 1) * chunk] + sums[2 * (d - 1) + side, :, where]
                for side in range(2)
            ])
        for side, block in enumerate(pair):
            settle(block, last, 1, raws[0][side], raws[1][side])
        state = attend_raw(state, (2 * d - 2, 2 * d - 1), *raws)

    highest, total, read = state
    head_of = lax.broadcasted_iota(jnp.int32, (MAP_ROWS, wide), 0) // 2
    own = jnp.zeros((MAP_ROWS, wide), jnp.float32)
    for h in range(heads):
        own = jnp.where(head_of == h, read[:, h * wide:(h + 1) * wide], own)
    lane_of = lax.broadcasted_iota(jnp.int32, (maps, wide), 1)
    stats[sp, core, 0] = own[:maps]
    stats[sp, core, 1] = jnp.where(
        lane_of == 0, highest[:maps], jnp.where(lane_of == 1, total[:maps], lam_row)
    )

    def stats_copy(target):
        d = lax.rem(target + n_sp - sp, n_sp)
        return pltpu.make_async_remote_copy(
            src_ref=stats.at[sp, core],
            dst_ref=stats.at[sp, core],
            send_sem=st_send.at[d],
            recv_sem=st_recv.at[d, core],
            device_id={"sp": target, "tp": tp + 1 - core},
            device_id_type=MESH,
        )

    def stats_arrival(d, source):
        return pltpu.make_async_remote_copy(
            src_ref=stats.at[sp, source],
            dst_ref=stats.at[sp, source],
            send_sem=st_send.at[d],
            recv_sem=st_recv.at[d, source],
            device_id={"tp": partner},
            device_id_type=MESH,
        )

    exchanges = []
    for k in range(n_sp - 1):
        up, down = k + jnp.where(k >= sp, 1, 0), n_sp - 1 - k - jnp.where(n_sp - 1 - k <= sp, 1, 0)
        exchanges.append(stats_copy(jnp.where(2 * sp >= n_sp, up, down)))
        exchanges[-1].start()
    pl.when(core == 0)(stats_copy(sp).start)

    def share_copy(d, target):
        chip = lax.rem(tp // 2 + d, chips)
        return pltpu.make_async_remote_copy(
            src_ref=part.at[d, target, pl.ds(0, 1)],
            dst_ref=parts.at[d, pl.ds(0, 1)],
            send_sem=pt_send.at[d, target],
            recv_sem=pt_recv.at[d],
            device_id={"tp": 2 * chip + target},
            device_id_type=MESH,
        )

    near.wait_send()
    pl.when(is_last)(to_helper.wait_send)

    @pl.when(is_helper)
    def _():
        for d in sources:
            relay_out_copy(d).wait_send()
            relay_back_copy(d).wait_send()

    for d in sources:
        for p in range(len(pieces) - 1):
            far_do(d, p, lambda copy: copy.wait_send())
    for copy in [*twins.values(), *forwards.values(), *exchanges]:
        copy.wait_send()

    @pl.when(is_lead)
    def _():
        own_wo.wait()
        lent_wo.wait_recv()
        stats_arrival(0, 0).wait_recv()
        for d in range(1, n_sp):
            for source in range(2):
                stats_arrival(d, source).wait_recv()
        headed, scales = [], []
        row_of = lax.broadcasted_iota(jnp.int32, (2 * MAP_ROWS, wide), 0)
        for c in range(2):
            heights = stats[:, c, 1]
            tops = heights[:, :, 0:1]
            totals = heights[:, :, 1:2]
            factor = jnp.exp(tops - jnp.max(tops, axis=0, keepdims=True))
            reads = jnp.sum(stats[:, c, 0] * factor, axis=0) / jnp.sum(totals * factor, axis=0)
            diff = reads - heights[0, :, 2:3] * pltpu.roll(reads, maps - 1, 0)
            scales.append(lax.rsqrt(jnp.mean(diff * diff, axis=1, keepdims=True) + 1e-06))
            gained = diff * gain[...]
            headed += [
                jnp.where(
                    row_of == c * MAP_ROWS + h, gained[2 * h:2 * h + 1], 0.0
                ).astype(jnp.bfloat16)
                for h in range(heads)
            ]
        headed = jnp.concatenate(headed, axis=1)
        for d in list(range(1, chips)) + [0]:
            for target in range(2):
                column = (2 * lax.rem(tp // 2 + d, chips) + target) * out_cols
                first = pl.multiple_of(column, out_cols)
                shares = jnp.dot(
                    headed, wo[:, pl.ds(first, out_cols)], preferred_element_type=jnp.float32
                )
                both = 0.0
                for c in range(2):
                    group = 0.0
                    for h in range(heads):
                        row = c * MAP_ROWS + h
                        group = group + shares[row:row + 1] * scales[c][2 * h:2 * h + 1]
                    both = both + group.astype(jnp.bfloat16).astype(jnp.float32)
                part[d, target, 0:1] = both
                if d > 0 or target == 0:
                    share_copy(d, target).start()
        mixed = part[0, 1, 0:1]
        for d in range(1, chips):
            share_copy(d, 1).wait_recv()
            mixed = mixed + parts[d, 0:1]
        mix_ref[...] = mixed.astype(jnp.bfloat16)
        for d in range(chips):
            for target in range(2):
                if d > 0 or target == 0:
                    share_copy(d, target).wait_send()

    @pl.when(core == 0)
    def _():
        lent_wo.wait_send()
        stats_copy(sp).wait_send()
        mixed = None
        for d in range(chips):
            share_copy(d, 1).wait_recv()
            mixed = parts[d, 0:1] if mixed is None else mixed + parts[d, 0:1]
        mix_ref[...] = mixed.astype(jnp.bfloat16)


def deliver(keys, values, mixed, key_out, value_out, mix_out, sem):
    copies = [
        pltpu.make_async_copy(source, target, sem.at[i])
        for i, (source, target) in enumerate(
            ((keys, key_out), (values, value_out), (mixed, mix_out))
        )
    ]
    for copy in copies:
        copy.start()
    for copy in copies:
        copy.wait()


def tables(length, chunk, head_dim):
    inverse = 1.0 / 10000.0 ** (np.arange(0, head_dim, 2) / head_dim)
    inverse = np.tile(inverse, 4)
    sign = np.tile(np.repeat([-1.0, 1.0], head_dim // 2), 2)

    def pair(positions, axis):
        angles = positions[:, None] * inverse[None, :]
        both = np.stack([np.cos(angles), np.sin(angles) * sign], axis=axis)
        return both.astype(np.float32)

    return pair(np.arange(chunk), 0), pair(np.arange(0, length, chunk), 1)


def on_device(n_sp, n_tp, x, key_weight, value_weight, new_queries, lambdas, head_gain, out_weight):
    heads = lambdas.shape[0]
    columns = key_weight.shape[1]
    head_dim = columns // (2 * heads)
    wide = 2 * head_dim
    seqs, rows, depth = x.shape
    assert seqs == 1 and n_sp > HELPER + 1
    chunk = rows // 4
    steps = rows // chunk
    chips = n_tp // 2
    pieces = steps - 1 + len(SLICES)
    out_cols = out_weight.shape[1] // n_tp
    fine, coarse = tables(n_sp * n_tp * rows, chunk, head_dim)
    hbm_spec = pl.BlockSpec(memory_space=pltpu.HBM)
    vmem_spec = pl.BlockSpec(memory_space=pltpu.VMEM)
    dma = pltpu.SemaphoreType.DMA
    bf16 = jnp.bfloat16
    f32 = jnp.float32
    room = 2 * n_tp * rows * columns * 2 + SMALL_BYTES
    cache = (n_tp, rows, columns)
    k, v, mixed = pl.pallas_call(
        functools.partial(kernel, n_sp, n_tp, heads, head_dim, chunk),
        out_shape=(
            pltpu.VMEM(cache, bf16),
            pltpu.VMEM(cache, bf16),
            pltpu.VMEM((1, out_cols), bf16),
        ),
        in_specs=[hbm_spec] * 9,
        out_specs=(vmem_spec,) * 3,
        scratch_shapes=[
            pltpu.VMEM((n_tp, rows, depth), bf16),
            pltpu.VMEM((depth, columns), bf16),
            pltpu.VMEM((depth, columns), bf16),
            pltpu.VMEM((2 * columns, out_weight.shape[1]), bf16),
            pltpu.VMEM((1, columns), bf16),
            pltpu.VMEM((1, heads), f32),
            pltpu.VMEM((1, wide), f32),
            pltpu.VMEM((2, chunk, wide), f32),
            pltpu.VMEM((n_tp * steps, 2, wide), f32),
            pltpu.VMEM((n_sp, 2, 2, 2 * heads, wide), f32),
            pltpu.VMEM((chips, 2, 8, out_cols), f32),
            pltpu.VMEM((chips, 8, out_cols), f32),
            pltpu.VMEM((2 * (chips - 1), chunk, 2 * columns), f32),
            pltpu.VMEM((2 * (chips - 1), chunk, columns), f32),
            pltpu.VMEM((columns, LANES), bf16),
            pltpu.VMEM((RELAY_ROWS, depth), bf16),
            pltpu.VMEM((chips - 1, RELAY_ROWS, depth), bf16),
            dma((9,)),
            dma((steps,)),
            pltpu.SemaphoreType.REGULAR,
            pltpu.SemaphoreType.REGULAR,
            dma,
            dma,
            dma((chips - 1, pieces - 1)),
            dma((chips - 1, pieces - 1)),
            dma((chips - 1, 2)),
            dma((chips - 1, 2)),
            dma((chips - 1, pieces - 1)),
            dma((chips - 1, pieces - 1)),
            dma,
            dma,
            dma((chips - 1,)),
            dma((chips - 1,)),
            dma((chips - 1,)),
            dma((chips - 1,)),
            dma,
            dma,
            dma((n_sp,)),
            dma((n_sp, 2)),
            dma((chips, 2)),
            dma((chips,)),
        ],
        compiler_params=pltpu.CompilerParams(
            collective_id=0, has_side_effects=True, vmem_limit_bytes=VMEM_BYTES - room
        ),
    )(
        x, key_weight, value_weight, new_queries, lambdas.reshape(1, heads),
        head_gain.reshape(1, wide), out_weight, jnp.asarray(fine), jnp.asarray(coarse),
    )
    k, v, mixed = pl.pallas_call(
        deliver,
        out_shape=(
            jax.ShapeDtypeStruct(cache, bf16),
            jax.ShapeDtypeStruct(cache, bf16),
            jax.ShapeDtypeStruct((1, out_cols), bf16),
        ),
        in_specs=[vmem_spec] * 3,
        out_specs=(hbm_spec,) * 3,
        scratch_shapes=[dma((3,))],
        compiler_params=pltpu.CompilerParams(vmem_limit_bytes=2**20),
    )(k, v, mixed)
    full = (1, n_tp * rows, columns)
    return k.reshape(full), v.reshape(full), mixed


def solution(mesh):
    n_sp, n_tp = mesh.shape["sp"], mesh.shape["tp"]
    in_specs = (
        P("gr", ("sp", "tp"), None),
        P(None, "tp"),
        P(None, "tp"),
        P("gr", "tp"),
        P("tp"),
        P(),
        P("tp", None),
    )
    out_specs = (P("gr", "sp", "tp"), P("gr", "sp", "tp"), P("gr", "tp"))
    return jax.shard_map(
        functools.partial(on_device, n_sp, n_tp),
        mesh=mesh, in_specs=in_specs, out_specs=out_specs, check_vma=False,
    )
```
